256 devices in a mesh: ep: 128 (over z, y, x), tp: 2 (over core).
Axes of the slice: x: 4, y: 4, z: 8, core: 2. Of those that a mesh axis runs over, the one named last changes fastest.
Arguments:
- tokens: bfloat16 [32768, 2048], P(('ep', 'tp')), may hold values from -6 to 6
- norm_gain: float32 [2048], replicated, may hold values from 0.25 to 4
- routes: int32 [32768, 2], P(('ep', 'tp')), may hold values from 0 to 127, all different within a row; in each aligned block of 128 rows (0 to 127, 128 to 255, ...) at most 3 rows name the same one
- route_weights: float32 [32768, 2], P(('ep', 'tp')), may hold values from 0.1 to 1
- w_gate: bfloat16 [128, 2048, 1024], P('ep', None, 'tp'), may hold values from -0.125 to 0.125
- w_up: bfloat16 [128, 2048, 1024], P('ep', None, 'tp'), may hold values from -0.125 to 0.125
- w_down: bfloat16 [128, 1024, 2048], P('ep', 'tp'), may hold values from -0.1875 to 0.1875
- dense_in: bfloat16 [2048, 256], P('ep'), may hold values from -0.125 to 0.125
- dense_out: bfloat16 [2048, 256], P('ep'), may hold values from -0.375 to 0.375
- dense_gate: float32 [2048], replicated, may hold values from -6 to 6
Outputs:
- mixed: bfloat16 [32768, 2048], P(('ep', 'tp'))
The draws below stay inside these ranges and needn't reach their ends.
Inputs may be any that keep to these rules, and one draw needn't show every extreme that they name: `routes`: each row names 2 different experts. Among the 128 rows of one device no expert is named more than 3 times; every draw has a device and an expert with exactly 3.
All inputs are finite; a program needn't handle non-finite values.
Results may differ from the reference program's by a relative error of at most 0.0074.
Values may be sent and summed in bfloat16 or wider, within the bound.
A program may use at most 128 MiB of HBM per device.

```python
import math
import jax
import jax.numpy as jnp
import numpy as np
from jax import lax

D = 2048
FF = 1024
DH = 256
TOP_K = 2
TOK_DEV = 128
EXPERTS = 128
TOKENS = 32768
CAP = 3
N_TP = 2


def draw_norm_gain(key, part):
    return 1.0 + 0.18 * jnp.clip(jax.random.normal(key, (D,), jnp.float32), -4.0, 4.0)


def shard_levels(key, shape, pieces, low, largest):
    factor_of = 1.0
    for axis_at, blocks in pieces:
        steps = jax.random.uniform(jax.random.fold_in(jax.random.fold_in(key, 6), axis_at), (blocks,), jnp.float32, low / len(pieces), largest / len(pieces))
        factor_of = factor_of * jnp.repeat(jnp.exp(steps), shape[axis_at] // blocks).reshape((-1,) + (1,) * (len(shape) - 1 - axis_at))
    return factor_of


def assign_block(own_key, own, number, rows, amount, top, bound, slope):
    order = jax.random.permutation(own_key, amount)
    packed, common = portions_of(amount, rows * top, bound, slope, True), portions_of(amount, rows * top, bound, slope, False)
    places = jnp.arange(amount)

    def named(lengths, turn):
        used = int((lengths > 0).sum())
        fixed = max(1, used // 4)
        passed = fixed + (places - fixed + turn * (used - fixed)) % max(1, amount - fixed)
        return jnp.zeros((amount,), jnp.int32).at[order[jnp.where(places < fixed, places, passed)]].set(jnp.asarray(lengths, jnp.int32))

    lengths = jnp.where(number % 4 == 0, named(packed, number // 4), named(common, number - number // 4 - 1))
    mixed = jax.random.permutation(jax.random.fold_in(own, 3), amount)
    donor, sink = mixed[0:amount // 2 * 2:2], mixed[1:amount // 2 * 2:2]
    margin = jnp.minimum(lengths[donor] - 1, bound - lengths[sink]) // 2
    margin = jnp.where((donor == order[0]) | (sink == order[0]) | (lengths[sink] == 0), 0, jnp.maximum(margin, 0))
    passed = jax.random.randint(jax.random.fold_in(own, 4), (amount // 2,), 0, 1 << 20) % (margin + 1)
    lengths = lengths.at[donor].add(-passed).at[sink].add(passed)
    items = jnp.searchsorted(jnp.cumsum(lengths), jnp.arange(rows * top), side="right").astype(jnp.int32)
    table = items.reshape(top, rows).T
    table = table[jax.random.permutation(jax.random.fold_in(own, 1), rows)]
    turn = jax.random.randint(jax.random.fold_in(own, 2), (rows, 1), 0, top)
    return jnp.take_along_axis(table, (jnp.arange(top)[None, :] + turn) % top, axis=1)


def portions_of(amount, total, reach, skew, full):
    loads = [(1 << 20) // math.isqrt(standing ** skew) + 1 for standing in range(1, amount + 1)]
    largest = reach if full else min(reach, max(-(-total // amount), total * loads[0] // sum(loads)))
    least = 1 if total - largest >= amount - 1 else 0
    given, spare = [largest] + [least] * (amount - 1), total - largest - least * (amount - 1)
    while spare > 0:
        free = [i for i in range(1, amount) if given[i] < largest] or [i for i in range(1, amount) if given[i] < reach]
        mass, left = sum([loads[i] for i in free]), spare
        for i in free:
            addition = min(reach - given[i], max(1, left * loads[i] // mass), spare)
            given[i] = given[i] + addition
            spare = spare - addition
    return np.array(given)


def noise(rng, dims, width, reach, split=(), kind=jnp.bfloat16):
    array = jax.random.normal(rng, dims, jnp.float32) * width
    if len(split) > 0:
        array = shard_levels(rng, dims, split, -0.22, 0.18) * array
    return jnp.clip(array, min=-reach, max=reach).astype(kind)


def setup_inputs(seed: int = 0) -> dict:
    key_of = jax.random.split(jax.random.key(seed), 11)
    tokens = noise(key_of[0], (TOKENS, D), 1.0, 6.0, ((0, 256),))
    norm_gain = draw_norm_gain(jax.random.fold_in(key_of[10], 71), 0)
    routes_keys = jax.random.split(jax.random.fold_in(key_of[2], 1), TOKENS // TOK_DEV)
    routes_turns = jax.random.permutation(jax.random.fold_in(key_of[2], 3), TOKENS // TOK_DEV)
    routes = jax.vmap(lambda own, number: assign_block(jax.random.fold_in(key_of[2], 2), own, number, TOK_DEV, EXPERTS, TOP_K, CAP, 2))(routes_keys, routes_turns).reshape((TOKENS, TOP_K))
    route_weights = jnp.clip(0.1 + 0.9 * jax.random.uniform(key_of[3], (TOKENS, TOP_K), jnp.float32) ** shard_levels(key_of[3], (TOKENS, TOP_K), ((0, 256),), -0.2, 0.2), 0.1, 1.0)
    w_gate = noise(key_of[4], (EXPERTS, D, FF), D ** -0.5, 0.125, ((0, 128), (2, 2)))
    w_up = noise(key_of[5], (EXPERTS, D, FF), D ** -0.5, 0.125, ((0, 128), (2, 2)))
    w_down = noise(key_of[6], (EXPERTS, FF, D), FF ** -0.5, 0.1875, ((0, 128), (1, 2)))
    dense_in = noise(key_of[7], (D, DH), D ** -0.5, 0.125, ((0, 128),))
    dense_out = noise(key_of[8], (D, DH), DH ** -0.5, 0.375, ((0, 128),))
    dense_gate = noise(key_of[9], (D,), 1.5, 6.0, (), jnp.float32)
    return dict(tokens=tokens, norm_gain=norm_gain, routes=routes, route_weights=route_weights, w_gate=w_gate, w_up=w_up, w_down=w_down, dense_in=dense_in, dense_out=dense_out, dense_gate=dense_gate)


CLAMP_LIMIT = 7.0
SLOPE_ALPHA = 1.702
NORM_EPS = 1e-06

def rms_normed(tokens, norm_gain):
    widened = tokens.astype(jnp.float32)
    inv_scale = lax.rsqrt(lax.optimization_barrier(jnp.mean(widened * widened, axis=1, keepdims=True)) + NORM_EPS)
    return (widened * inv_scale * norm_gain).astype(jnp.bfloat16)

def clamped_unit(gate_pre, up_pre):
    gate_clip = jnp.minimum(gate_pre, CLAMP_LIMIT)
    up_clip = jnp.clip(up_pre, -CLAMP_LIMIT, CLAMP_LIMIT)
    return ((up_clip + 1.0) * gate_clip * jax.nn.sigmoid(SLOPE_ALPHA * gate_clip)).astype(jnp.bfloat16)

def reference(tokens, norm_gain, routes, route_weights, w_gate, w_up, w_down, dense_in, dense_out, dense_gate):
    normed = rms_normed(tokens, norm_gain)
    sources = TOKENS // TOK_DEV
    entries = TOK_DEV * TOP_K
    block_routes = routes.reshape(sources, entries)
    onehot = (block_routes[:, :, None] == jnp.arange(EXPERTS, dtype=jnp.int32)[None, None, :]).astype(jnp.int32)
    slot_index = lax.optimization_barrier(jnp.sum((jnp.cumsum(onehot, axis=1) - onehot) * onehot, axis=2))
    source_ids = jnp.arange(sources, dtype=jnp.int32)[:, None]
    position = (block_routes * (sources * CAP) + source_ids * CAP + slot_index).reshape(-1).astype(jnp.int32)
    entry_ids = jnp.arange(TOKENS * TOP_K, dtype=jnp.int32)
    slot_table = jnp.full((EXPERTS * sources * CAP,), -1, jnp.int32).at[position].set(entry_ids)
    slot_table = slot_table.reshape(EXPERTS, sources * CAP)
    half_width = FF // N_TP

    def one_expert(expert_args):
        entry_index, gate_w, up_w, down_w = expert_args
        is_valid = entry_index >= 0
        token_of = jnp.where(is_valid, entry_index, 0) // TOP_K
        gathered_rows = jnp.where(is_valid[:, None], normed[token_of], jnp.zeros((), jnp.bfloat16))
        gate_pre = jnp.dot(gathered_rows, gate_w, preferred_element_type=jnp.float32)
        up_pre = jnp.dot(gathered_rows, up_w, preferred_element_type=jnp.float32)
        hidden = clamped_unit(gate_pre, up_pre)
        summed = jnp.zeros((gathered_rows.shape[0], D), jnp.float32)
        for half_index in range(N_TP):
            low = half_index * half_width
            partial_value = jnp.dot(hidden[:, low:low + half_width], down_w[low:low + half_width], preferred_element_type=jnp.float32).astype(jnp.bfloat16)
            summed = summed + lax.optimization_barrier(partial_value).astype(jnp.float32)
        return summed.astype(jnp.bfloat16)
    results = lax.map(one_expert, (slot_table, w_gate, w_up, w_down))
    flat_results = results.reshape(EXPERTS * sources * CAP, D)
    picked = flat_results[position].astype(jnp.float32).reshape(TOKENS, TOP_K, D)
    weighted = lax.optimization_barrier(jnp.sum(picked * route_weights[:, :, None], axis=1))
    dense_hidden = jax.nn.silu(jnp.dot(normed, dense_in, preferred_element_type=jnp.float32)).astype(jnp.bfloat16)
    branch = lax.dot_general(dense_hidden, dense_out, (((1,), (1,)), ((), ())), preferred_element_type=jnp.float32)
    return (weighted + jax.nn.sigmoid(dense_gate) * branch).astype(jnp.bfloat16)
```

```python
import jax
import jax.numpy as jnp
from jax import lax
from jax.experimental import pallas as pl
from jax.experimental.pallas import tpu as pltpu
from jax.sharding import PartitionSpec as P

CLAMP_LIMIT = 7.0
SLOPE_ALPHA = 1.702
NORM_EPS = 1e-06
MESH = pl.DeviceIdType.MESH
BF16 = jnp.bfloat16
F32 = jnp.float32

PEERS = 128
CAP = 3
LANES = 128
SUB = 16
SELF = 7
GROUPS = 2
PER_GROUP = PEERS // GROUPS
ROWS = PER_GROUP * CAP
PACK = 16


def place_of(dz, dy, dx):
    j = jnp.where(dz == 0, 0, jnp.where(dz <= 4, 2 * dz - 1, 2 * (8 - dz)))
    return (dy * 4 + dx) * 8 + 7 - j


def offset_of(k):
    j = 7 - lax.rem(k, 8)
    odd = lax.rem(j, 2)
    half = lax.div(j, 2)
    dz = lax.rem(odd * (half + 1) + (1 - odd) * (8 - half), 8)
    r = lax.div(k, 8)
    return dz, lax.div(r, 4), lax.rem(r, 4)


def clamped_unit(gate_pre, up_pre):
    gate_clip = jnp.minimum(gate_pre, CLAMP_LIMIT)
    up_clip = jnp.clip(up_pre, -CLAMP_LIMIT, CLAMP_LIMIT)
    return ((up_clip + 1.0) * gate_clip * jax.nn.sigmoid(SLOPE_ALPHA * gate_clip)).astype(BF16)


def kernel(
    src_ref, pos_ref, rw_ref, tok_hbm, gain_ref, dgate_ref, wg_hbm, wu_hbm, wd_hbm, din_hbm, dout_hbm,
    o_ref,
    tok, x2, x3, send, recv, xg, hid, acc, outb, ret, wg, wu, wd, wgo, wuo, wdo, dense, branch,
    tok_sem, w_sem, wsend_sem, wrecv_sem, d_sem, dsend_sem, drecv_sem,
    send_sem, recv_sem, rsend_sem, rrecv_sem,
):
    me = lax.axis_index("ep")
    tp = lax.axis_index("tp")
    z, y, x = lax.div(me, 16), lax.rem(lax.div(me, 4), 4), lax.rem(me, 4)

    def chip(dz, dy, dx):
        return (
            lax.rem(z + dz, 8) * 16 + lax.rem(y + dy, 4) * 4 + lax.rem(x + dx, 4)
        )

    def back(dz, dy, dx):
        return (
            lax.rem(z + 8 - dz, 8) * 16 + lax.rem(y + 4 - dy, 4) * 4 + lax.rem(x + 4 - dx, 4)
        )

    tok_copy = pltpu.make_async_copy(tok_hbm, tok, tok_sem)
    tok_copy.start()

    @pl.when(tp == 0)
    def _():
        pltpu.make_async_copy(din_hbm, dense.at[0, z, y, x], d_sem).start()

    @pl.when(tp == 1)
    def _():
        pltpu.make_async_copy(dout_hbm, dense.at[1, z, y, x], d_sem).start()

    barrier = pltpu.get_barrier_semaphore()

    def greet(k, c):
        pl.semaphore_signal(
            barrier, inc=1, device_id=(lax.rem(me + k, PEERS), tp), device_id_type=MESH
        )
        return c

    lax.fori_loop(1, PEERS, greet, 0)
    pl.semaphore_signal(barrier, inc=1, device_id=(me, 1 - tp), device_id_type=MESH)

    own = [
        pltpu.make_async_copy(a, b, w_sem.at[i])
        for i, (a, b) in enumerate(((wg_hbm, wg), (wu_hbm, wu), (wd_hbm, wd)))
    ]
    other = [
        pltpu.make_async_remote_copy(
            src_ref=a, dst_ref=b, send_sem=wsend_sem.at[i], recv_sem=wrecv_sem.at[i],
            device_id=(me, 1 - tp), device_id_type=MESH,
        )
        for i, (a, b) in enumerate(((wg_hbm, wgo), (wu_hbm, wuo), (wd_hbm, wdo)))
    ]

    tok_copy.wait()
    for copy in own:
        copy.start()

    for i in range(8):
        rows = slice(i * 16, i * 16 + 16)
        wide = tok[rows, :].astype(F32)
        scale = lax.rsqrt(jnp.mean(wide * wide, axis=1, keepdims=True) + NORM_EPS)
        normed = (wide * scale * gain_ref[...]).astype(BF16)
        x2[rows, :] = normed
        x3[rows] = normed.reshape(16, SUB, LANES)

    pltpu.make_async_copy(din_hbm, dense.at[tp, z, y, x], d_sem).wait()
    pl.semaphore_wait(barrier, PEERS)

    def spread(stage, count, block, target):
        def one(d, c):
            pltpu.make_async_remote_copy(
                src_ref=block, dst_ref=block, send_sem=dsend_sem.at[stage],
                recv_sem=drecv_sem.at[stage], device_id=(target(d), tp), device_id_type=MESH,
            ).start()
            return c

        lax.fori_loop(1, count, one, 0)

    z_block = dense.at[tp, z, y, x]
    y_block = dense.at[tp, :, y, x]
    x_block = dense.at[tp, :, :, x]
    z_all = dense.at[tp, pl.ds(0, 7), y, x]
    y_all = dense.at[tp, :, pl.ds(0, 3), x]
    x_all = dense.at[tp, :, :, pl.ds(0, 3)]

    def all_in(ref, sem):
        pltpu.make_async_copy(ref, ref, sem).wait()

    spread(0, 8, z_block, lambda d: chip(d, 0, 0))

    def pack(k, c):
        for s in range(CAP):
            send[k * CAP + s] = x3[src_ref[k * CAP + s]]
        return c

    def dispatch(k, c):
        rows = pl.ds(k * CAP, CAP)

        @pl.when(k != SELF)
        def _():
            pltpu.make_async_remote_copy(
                src_ref=send.at[rows], dst_ref=recv.at[rows], send_sem=send_sem,
                recv_sem=recv_sem.at[lax.div(k, PER_GROUP)],
                device_id=(chip(*offset_of(k)), tp), device_id_type=MESH,
            ).start()

        return c

    def pack_and_send(first, last):
        lax.fori_loop(first, first + PACK, pack, 0)

        def step(b, c):
            lax.fori_loop(b * PACK + PACK, b * PACK + 2 * PACK, pack, 0)
            lax.fori_loop(b * PACK, b * PACK + PACK, dispatch, 0)
            return c

        lax.fori_loop(first // PACK, last // PACK - 1, step, 0)
        lax.fori_loop(last - PACK, last, dispatch, 0)

    pack_and_send(0, PER_GROUP)
    for s in range(CAP):
        recv[SELF * CAP + s] = send[SELF * CAP + s]

    all_in(z_all, drecv_sem.at[0])
    spread(1, 4, y_block, lambda d: chip(0, d, 0))
    pack_and_send(PER_GROUP, PEERS)
    for copy in other:
        copy.start()
    all_in(y_all, drecv_sem.at[1])
    spread(2, 4, x_block, lambda d: chip(0, 0, d))

    def answer(k, c):
        rows = pl.ds(k * CAP, CAP)

        @pl.when(k != SELF)
        def _():
            pltpu.make_async_remote_copy(
                src_ref=outb.at[rows], dst_ref=ret.at[rows], send_sem=rsend_sem,
                recv_sem=rrecv_sem.at[lax.div(k, PER_GROUP)],
                device_id=(back(*offset_of(k)), tp), device_id_type=MESH,
            ).start()

        return c

    def group_bytes(g):
        return PER_GROUP - 1 if g == 0 else PER_GROUP

    for g in range(GROUPS):
        base = g * ROWS
        all_in(recv.at[pl.ds(0, group_bytes(g) * CAP)], recv_sem.at[g])

        for r in range(0, ROWS, 16):
            xg[r : r + 16, :] = recv[base + r : base + r + 16].reshape(16, SUB * LANES)

        for h, (gate_w, up_w) in enumerate(((wg, wu), (wgo, wuo))):
            if g == 0:
                if h == 0:
                    for copy in own:
                        copy.wait()
                else:
                    for copy in other:
                        copy.wait_recv()
            for t in range(2):
                cols = slice(t * 256, t * 256 + 256)
                hid[:, h * 512 + t * 256 : h * 512 + t * 256 + 256] = clamped_unit(
                    jnp.dot(xg[...], gate_w[:, cols], preferred_element_type=F32),
                    jnp.dot(xg[...], up_w[:, cols], preferred_element_type=F32),
                )

        for t in range(8):
            cols = slice(t * 256, t * 256 + 256)
            first = jnp.dot(hid[:, :512], wd[:, cols], preferred_element_type=F32).astype(BF16)
            second = jnp.dot(hid[:, 512:], wdo[:, cols], preferred_element_type=F32).astype(BF16)
            summed = first.astype(F32) + second.astype(F32)
            for i in range(2):
                acc[pl.ds(2 * t + i, ROWS, stride=SUB), :] = summed[:, i * LANES : (i + 1) * LANES]

        for r in range(0, ROWS, 16):
            outb[base + r : base + r + 16] = (
                acc[r * SUB : (r + 16) * SUB, :].reshape(16, SUB, LANES).astype(BF16)
            )

        lax.fori_loop(g * PER_GROUP, (g + 1) * PER_GROUP, answer, 0)

    for s in range(CAP):
        ret[SELF * CAP + s] = outb[SELF * CAP + s]

    all_in(x_all, drecv_sem.at[2])
    swap = pltpu.make_async_remote_copy(
        src_ref=dense.at[tp], dst_ref=dense.at[tp], send_sem=dsend_sem.at[3],
        recv_sem=drecv_sem.at[3], device_id=(me, 1 - tp), device_id_type=MESH,
    )
    swap.start()
    swap.wait_recv()

    pre = jnp.zeros((128, 256), F32)
    for i in range(8):
        pre = pre + jnp.dot(
            x2[:, i * 256 : (i + 1) * 256], dense[0, i].reshape(256, 256), preferred_element_type=F32
        )
    dense_hidden = jax.nn.silu(pre).astype(BF16)
    for i in range(8):
        part = lax.dot_general(
            dense_hidden, dense[1, i].reshape(256, 256), (((1,), (1,)), ((), ())),
            preferred_element_type=F32,
        )
        for j in range(2):
            branch[pl.ds(2 * i + j, 128, stride=SUB), :] = part[:, j * LANES : (j + 1) * LANES]

    gate = jax.nn.sigmoid(dgate_ref[...])
    for g in range(GROUPS):
        all_in(ret.at[pl.ds(0, group_bytes(g) * CAP)], rrecv_sem.at[g])

    @pl.loop(0, 128)
    def _(t):
        weighted = (
            rw_ref[2 * t] * ret[pos_ref[2 * t]].astype(F32)
            + rw_ref[2 * t + 1] * ret[pos_ref[2 * t + 1]].astype(F32)
        )
        tile = pl.ds(pl.multiple_of(t * SUB, SUB), SUB)
        o_ref[t] = (weighted + gate * branch[tile, :]).astype(BF16)

    all_in(send.at[pl.ds(0, (PEERS - 1) * CAP)], send_sem)
    all_in(outb.at[pl.ds(0, (PEERS - 1) * CAP)], rsend_sem)
    for copy in other:
        copy.wait_send()
    all_in(z_all, dsend_sem.at[0])
    all_in(y_all, dsend_sem.at[1])
    all_in(x_all, dsend_sem.at[2])
    swap.wait_send()


def tables(routes):
    rows, top = routes.shape
    entries = rows * top
    me = lax.axis_index("ep")
    flat = routes.reshape(entries)
    onehot = flat[:, None] == lax.broadcasted_iota(jnp.int32, (1, PEERS), 1)
    earlier = (
        lax.broadcasted_iota(jnp.int32, (entries, entries), 0)
        > lax.broadcasted_iota(jnp.int32, (entries, entries), 1)
    ).astype(BF16)
    counted = jnp.dot(earlier, onehot.astype(BF16), preferred_element_type=F32)
    slot = jnp.sum(jnp.where(onehot, counted, 0.0), axis=1).astype(jnp.int32)
    dz = (flat // 16 - me // 16) % 8
    dy = (flat // 4 % 4 - me // 4 % 4) % 4
    dx = (flat % 4 - me % 4) % 4
    position = place_of(dz, dy, dx) * CAP + slot
    places = position[None, :] == lax.broadcasted_iota(jnp.int32, (PEERS * CAP, 1), 0)
    source = jnp.sum(
        jnp.where(places, lax.broadcasted_iota(jnp.int32, (1, entries), 1) // top, 0), axis=1
    )
    return source, position


def shards(
    tokens, norm_gain, routes, route_weights, w_gate, w_up, w_down, dense_in, dense_out, dense_gate
):
    source, position = tables(routes)
    smem = pl.BlockSpec(memory_space=pltpu.SMEM)
    vmem = pl.BlockSpec(memory_space=pltpu.VMEM)
    hbm = pl.BlockSpec(memory_space=pl.ANY)
    dma = pltpu.SemaphoreType.DMA
    out = pl.pallas_call(
        kernel,
        out_shape=jax.ShapeDtypeStruct((128, SUB, LANES), BF16),
        in_specs=[smem, smem, smem, hbm, vmem, vmem, hbm, hbm, hbm, hbm, hbm],
        out_specs=vmem,
        scratch_shapes=[
            pltpu.VMEM((128, 2048), BF16),
            pltpu.VMEM((128, 2048), BF16),
            pltpu.VMEM((128, SUB, LANES), BF16),
            pltpu.VMEM((PEERS * CAP, SUB, LANES), BF16),
            pltpu.VMEM((PEERS * CAP, SUB, LANES), BF16),
            pltpu.VMEM((ROWS, 2048), BF16),
            pltpu.VMEM((ROWS, 1024), BF16),
            pltpu.VMEM((ROWS * SUB, LANES), F32),
            pltpu.VMEM((PEERS * CAP, SUB, LANES), BF16),
            pltpu.VMEM((PEERS * CAP, SUB, LANES), BF16),
            pltpu.VMEM((2048, 512), BF16),
            pltpu.VMEM((2048, 512), BF16),
            pltpu.VMEM((512, 2048), BF16),
            pltpu.VMEM((2048, 512), BF16),
            pltpu.VMEM((2048, 512), BF16),
            pltpu.VMEM((512, 2048), BF16),
            pltpu.VMEM((2, 8, 4, 4, 16, 256), BF16),
            pltpu.VMEM((128 * SUB, LANES), F32),
            dma, dma((3,)), dma((3,)), dma((3,)), dma, dma((4,)), dma((4,)),
            dma, dma((GROUPS,)), dma, dma((GROUPS,)),
        ],
        compiler_params=pltpu.CompilerParams(
            collective_id=0, has_side_effects=True, vmem_limit_bytes=56 << 20
        ),
    )(
        source, position, route_weights.reshape(-1), tokens, norm_gain.reshape(1, -1),
        dense_gate.reshape(SUB, LANES), w_gate[0], w_up[0], w_down[0], dense_in, dense_out,
    )
    return out.reshape(tokens.shape)


def solution(mesh):
    placed = (
        P(("ep", "tp"), None),
        P(),
        P(("ep", "tp"), None),
        P(("ep", "tp"), None),
        P("ep", None, "tp"),
        P("ep", None, "tp"),
        P("ep", "tp", None),
        P("ep", None),
        P("ep", None),
        P(),
    )
    return jax.shard_map(
        shards, mesh=mesh, in_specs=placed, out_specs=P(("ep", "tp"), None), check_vma=False
    )
```

```python
import jax
import jax.numpy as jnp
from jax import lax
from jax.experimental import pallas as pl
from jax.experimental.pallas import tpu as pltpu
from jax.sharding import PartitionSpec as P

CLAMP_LIMIT = 7.0
SLOPE_ALPHA = 1.702
NORM_EPS = 1e-06
MESH = pl.DeviceIdType.MESH
BF16 = jnp.bfloat16
F32 = jnp.float32

PEERS = 128
CAP = 3
LANES = 128
SUB = 16
SELF = 7
GROUPS = 2
PER_GROUP = PEERS // GROUPS
ROWS = PER_GROUP * CAP
PACK = 16


def place_of(dz, dy, dx):
    j = jnp.where(dz == 0, 0, jnp.where(dz <= 4, 2 * dz - 1, 2 * (8 - dz)))
    return (dx * 4 + dy) * 8 + 7 - j


def offset_of(k):
    j = 7 - lax.rem(k, 8)
    odd = lax.rem(j, 2)
    half = lax.div(j, 2)
    dz = lax.rem(odd * (half + 1) + (1 - odd) * (8 - half), 8)
    r = lax.div(k, 8)
    return dz, lax.rem(r, 4), lax.div(r, 4)


def clamped_unit(gate_pre, up_pre):
    gate_clip = jnp.minimum(gate_pre, CLAMP_LIMIT)
    up_clip = jnp.clip(up_pre, -CLAMP_LIMIT, CLAMP_LIMIT)
    return ((up_clip + 1.0) * gate_clip * jax.nn.sigmoid(SLOPE_ALPHA * gate_clip)).astype(BF16)


def kernel(
    routes_hbm, rw_hbm, tok_hbm, gain_hbm, dgate_hbm, wg_hbm, wu_hbm, wd_hbm, din_hbm, dout_hbm,
    o_hbm,
    routes, gain, dgate, table, index, rw,
    tok, x2, x3, send, recv, xg, hid, acc, outb, ret, wg, wu, wd, wgo, wuo, wdo, dense, branch, out2,
    small_sem, index_sem, y_sem, x_sem, out_sem,
    tok_sem, w_sem, wsend_sem, wrecv_sem, d_sem, dsend_sem, drecv_sem,
    send_sem, recv_sem, rsend_sem, rrecv_sem,
):
    me = lax.axis_index("ep")
    tp = lax.axis_index("tp")
    z, y, x = lax.div(me, 16), lax.rem(lax.div(me, 4), 4), lax.rem(me, 4)

    def chip(dz, dy, dx):
        return (
            lax.rem(z + dz, 8) * 16 + lax.rem(y + dy, 4) * 4 + lax.rem(x + dx, 4)
        )

    def back(dz, dy, dx):
        return (
            lax.rem(z + 8 - dz, 8) * 16 + lax.rem(y + 4 - dy, 4) * 4 + lax.rem(x + 4 - dx, 4)
        )

    small = [
        pltpu.make_async_copy(a, b, small_sem.at[i])
        for i, (a, b) in enumerate(
            ((routes_hbm, routes), (gain_hbm, gain), (rw_hbm, rw), (dgate_hbm, dgate))
        )
    ]
    tok_copy = pltpu.make_async_copy(tok_hbm, tok, tok_sem)
    small[0].start()
    tok_copy.start()

    def greet(sem, device):
        pl.semaphore_signal(sem, inc=1, device_id=device, device_id_type=MESH)

    barrier = pltpu.get_barrier_semaphore()
    for d in (4, 3, 5, 2, 6, 1, 7):
        greet(barrier, (chip(d, 0, 0), tp))
    for d in (2, 1, 3):
        greet(barrier, (chip(0, d, 0), tp))
        greet(barrier, (chip(0, 0, d), tp))
    greet(barrier, (me, 1 - tp))
    for copy in small[1:]:
        copy.start()

    @pl.when(tp == 0)
    def _():
        pltpu.make_async_copy(din_hbm, dense.at[0, z, y, x], d_sem).start()

    @pl.when(tp == 1)
    def _():
        pltpu.make_async_copy(dout_hbm, dense.at[1, z, y, x], d_sem).start()

    own = [
        pltpu.make_async_copy(a, b, w_sem.at[i])
        for i, (a, b) in enumerate(((wg_hbm, wg), (wu_hbm, wu), (wd_hbm, wd)))
    ]
    other = [
        pltpu.make_async_remote_copy(
            src_ref=a, dst_ref=b, send_sem=wsend_sem.at[i], recv_sem=wrecv_sem.at[i],
            device_id=(me, 1 - tp), device_id_type=MESH,
        )
        for i, (a, b) in enumerate(((wg_hbm, wgo), (wu_hbm, wuo), (wd_hbm, wdo)))
    ]

    table[...] = jnp.zeros_like(table)
    small[0].wait()
    chosen = routes[...]
    place = place_of(
        (lax.shift_right_logical(chosen, 4) - z) & 7,
        ((lax.shift_right_logical(chosen, 2) & 3) - y) & 3,
        ((chosen & 3) - x) & 3,
    )
    sub = lax.broadcasted_iota(jnp.int32, (PEERS, 128), 0)
    lane = lax.broadcasted_iota(jnp.int32, (PEERS, 128), 1)
    before = jnp.where(sub < lane, 1.0, 0.0).astype(BF16)
    token = lax.broadcasted_iota(jnp.int32, (8, 128), 1).astype(F32).astype(BF16)
    hits, slots = [], []
    for c in range(2):
        hit = jnp.where(sub == place[c : c + 1, :], 1.0, 0.0)
        earlier = jnp.dot(hit.astype(BF16), before, preferred_element_type=F32)
        if c == 1:
            earlier = earlier + jnp.sum(hits[0], axis=1, keepdims=True)
        slot = jnp.sum(hit * earlier, axis=0, keepdims=True)
        table[3 + c : 4 + c, :] = jnp.clip(
            place[c : c + 1, :] * CAP + slot.astype(jnp.int32), 0, PEERS * CAP - 1
        )
        hits.append(hit)
        slots.append(slot)
    for s in range(CAP):
        held = sum(jnp.where(slots[c] == s, hits[c], 0.0) for c in range(2)).astype(BF16)
        named = lax.dot_general(
            token, held, (((1,), (1,)), ((), ())), preferred_element_type=F32
        )
        table[s : s + 1, :] = jnp.clip(named[:1].astype(jnp.int32), 0, 127)
    index_copy = pltpu.make_async_copy(table, index, index_sem)
    index_copy.start()

    pl.semaphore_wait(barrier, 14)
    for d in (2, 1, 3):
        greet(y_sem, (chip(0, d, 0), tp))

    tok_copy.wait()
    for copy in own:
        copy.start()
    small[1].wait()
    for i in range(8):
        rows = slice(i * 16, i * 16 + 16)
        wide = tok[rows, :].astype(F32)
        scale = lax.rsqrt(jnp.mean(wide * wide, axis=1, keepdims=True) + NORM_EPS)
        normed = (wide * scale * gain[...]).astype(BF16)
        x2[rows, :] = normed
        x3[rows] = normed.reshape(16, SUB, LANES)
    pltpu.make_async_copy(din_hbm, dense.at[tp, z, y, x], d_sem).wait()
    index_copy.wait()

    def spread(stage, count, block, target):
        for d in range(1, count):
            pltpu.make_async_remote_copy(
                src_ref=block, dst_ref=block, send_sem=dsend_sem.at[stage],
                recv_sem=drecv_sem.at[stage], device_id=(target(d), tp), device_id_type=MESH,
            ).start()

    def along_y(d):
        return chip(0, d, 0)

    def along_x(d):
        return chip(0, 0, d)

    z_all = dense.at[tp, pl.ds(0, 7), y, x]
    second_all = dense.at[tp, :, pl.ds(0, 3), x]
    third_all = dense.at[tp, :, :, pl.ds(0, 3)]

    def all_in(ref, sem):
        pltpu.make_async_copy(ref, ref, sem).wait()

    def pack(k, c):
        for s in range(CAP):
            send[k * CAP + s] = x3[index[s, k]]
        return c

    def dispatch(k, c):
        rows = pl.ds(k * CAP, CAP)

        @pl.when(k != SELF)
        def _():
            pltpu.make_async_remote_copy(
                src_ref=send.at[rows], dst_ref=recv.at[rows], send_sem=send_sem,
                recv_sem=recv_sem.at[lax.div(k, PER_GROUP)],
                device_id=(chip(*offset_of(k)), tp), device_id_type=MESH,
            ).start()

        return c

    lax.fori_loop(0, 32, pack, 0)
    lax.fori_loop(0, 8, dispatch, 0)
    spread(0, 8, dense.at[tp, z, y, x], lambda d: chip(d, 0, 0))
    pl.semaphore_wait(y_sem, 3)
    for d in (2, 1, 3):
        greet(x_sem, (chip(0, 0, d), tp))
    lax.fori_loop(8, 32, dispatch, 0)
    lax.fori_loop(32, 64, pack, 0)
    pl.semaphore_wait(x_sem, 3)
    lax.fori_loop(32, 64, dispatch, 0)
    lax.fori_loop(64, 128, pack, 0)
    for s in range(CAP):
        recv[SELF * CAP + s] = send[SELF * CAP + s]

    all_in(z_all, drecv_sem.at[0])

    @pl.when(tp == 0)
    def _():
        spread(1, 4, dense.at[0, :, y, x], along_y)

    @pl.when(tp == 1)
    def _():
        spread(1, 4, dense.at[1, :, y, x], along_x)

    lax.fori_loop(64, 128, dispatch, 0)
    for copy in other:
        copy.start()
    all_in(second_all, drecv_sem.at[1])

    @pl.when(tp == 0)
    def _():
        spread(2, 4, dense.at[0, :, :, x], along_x)

    @pl.when(tp == 1)
    def _():
        spread(2, 4, dense.at[1, :, y], along_y)

    def answer(k, c):
        rows = pl.ds(k * CAP, CAP)

        @pl.when(k != SELF)
        def _():
            pltpu.make_async_remote_copy(
                src_ref=outb.at[rows], dst_ref=ret.at[rows], send_sem=rsend_sem,
                recv_sem=rrecv_sem.at[lax.div(k, PER_GROUP)],
                device_id=(back(*offset_of(k)), tp), device_id_type=MESH,
            ).start()

        return c

    def group_bytes(g):
        return PER_GROUP - 1 if g == 0 else PER_GROUP

    for g in range(GROUPS):
        base = g * ROWS
        all_in(recv.at[pl.ds(0, group_bytes(g) * CAP)], recv_sem.at[g])

        for r in range(0, ROWS, 16):
            xg[r : r + 16, :] = recv[base + r : base + r + 16].reshape(16, SUB * LANES)

        for h, (gate_w, up_w) in enumerate(((wg, wu), (wgo, wuo))):
            if g == 0:
                if h == 0:
                    for copy in own:
                        copy.wait()
                else:
                    for copy in other:
                        copy.wait_recv()
            for t in range(2):
                cols = slice(t * 256, t * 256 + 256)
                hid[:, h * 512 + t * 256 : h * 512 + t * 256 + 256] = clamped_unit(
                    jnp.dot(xg[...], gate_w[:, cols], preferred_element_type=F32),
                    jnp.dot(xg[...], up_w[:, cols], preferred_element_type=F32),
                )

        for t in range(8):
            cols = slice(t * 256, t * 256 + 256)
            first = jnp.dot(hid[:, :512], wd[:, cols], preferred_element_type=F32).astype(BF16)
            second = jnp.dot(hid[:, 512:], wdo[:, cols], preferred_element_type=F32).astype(BF16)
            summed = first.astype(F32) + second.astype(F32)
            for i in range(2):
                acc[pl.ds(2 * t + i, ROWS, stride=SUB), :] = summed[:, i * LANES : (i + 1) * LANES]

        for r in range(0, ROWS, 16):
            outb[base + r : base + r + 16] = (
                acc[r * SUB : (r + 16) * SUB, :].reshape(16, SUB, LANES).astype(BF16)
            )

        lax.fori_loop(g * PER_GROUP, (g + 1) * PER_GROUP, answer, 0)

    for s in range(CAP):
        ret[SELF * CAP + s] = outb[SELF * CAP + s]

    all_in(third_all, drecv_sem.at[2])
    swap = pltpu.make_async_remote_copy(
        src_ref=dense.at[tp], dst_ref=dense.at[tp], send_sem=dsend_sem.at[3],
        recv_sem=drecv_sem.at[3], device_id=(me, 1 - tp), device_id_type=MESH,
    )
    swap.start()
    swap.wait_recv()

    pre = jnp.zeros((128, 256), F32)
    for i in range(8):
        pre = pre + jnp.dot(
            x2[:, i * 256 : (i + 1) * 256], dense[0, i].reshape(256, 256), preferred_element_type=F32
        )
    dense_hidden = jax.nn.silu(pre).astype(BF16)
    small[3].wait()
    gate = jax.nn.sigmoid(dgate[...])
    for i in range(8):
        part = lax.dot_general(
            dense_hidden, dense[1, i].reshape(256, 256), (((1,), (1,)), ((), ())),
            preferred_element_type=F32,
        )
        for j in range(2):
            at = 2 * i + j
            branch[pl.ds(at, 128, stride=SUB), :] = (
                part[:, j * LANES : (j + 1) * LANES] * gate[at : at + 1, :]
            )

    small[2].wait()
    for g in range(GROUPS):
        all_in(ret.at[pl.ds(0, group_bytes(g) * CAP)], rrecv_sem.at[g])

    def combine(t, c):
        tile = pl.ds(pl.multiple_of(t * SUB, SUB), SUB)
        acc[tile, :] = (
            rw[0, t] * ret[index[3, t]].astype(F32) + rw[1, t] * ret[index[4, t]].astype(F32)
        ) + branch[tile, :]
        return c

    for r in range(0, 128, 16):
        lax.fori_loop(r, r + 16, combine, 0, unroll=8)
        out2[r : r + 16, :] = (
            acc[r * SUB : (r + 16) * SUB, :].reshape(16, SUB * LANES).astype(BF16)
        )
        pltpu.make_async_copy(out2.at[r : r + 16], o_hbm.at[r : r + 16], out_sem).start()
    pltpu.make_async_copy(out2, o_hbm, out_sem).wait()

    all_in(send.at[pl.ds(0, (PEERS - 1) * CAP)], send_sem)
    all_in(outb.at[pl.ds(0, (PEERS - 1) * CAP)], rsend_sem)
    for copy in other:
        copy.wait_send()
    all_in(z_all, dsend_sem.at[0])
    all_in(second_all, dsend_sem.at[1])
    all_in(third_all, dsend_sem.at[2])
    swap.wait_send()


def shards(
    tokens, norm_gain, routes, route_weights, w_gate, w_up, w_down, dense_in, dense_out, dense_gate
):
    hbm = pl.BlockSpec(memory_space=pl.ANY)
    dma = pltpu.SemaphoreType.DMA
    return pl.pallas_call(
        kernel,
        out_shape=jax.ShapeDtypeStruct((128, 2048), BF16),
        in_specs=[hbm] * 10,
        out_specs=hbm,
        scratch_shapes=[
            pltpu.VMEM((2, 128), jnp.int32),
            pltpu.VMEM((1, 2048), F32),
            pltpu.VMEM((SUB, LANES), F32),
            pltpu.VMEM((8, 128), jnp.int32),
            pltpu.SMEM((8, 128), jnp.int32),
            pltpu.SMEM((2, 128), F32),
            pltpu.VMEM((128, 2048), BF16),
            pltpu.VMEM((128, 2048), BF16),
            pltpu.VMEM((128, SUB, LANES), BF16),
            pltpu.VMEM((PEERS * CAP, SUB, LANES), BF16),
            pltpu.VMEM((PEERS * CAP, SUB, LANES), BF16),
            pltpu.VMEM((ROWS, 2048), BF16),
            pltpu.VMEM((ROWS, 1024), BF16),
            pltpu.VMEM((ROWS * SUB, LANES), F32),
            pltpu.VMEM((PEERS * CAP, SUB, LANES), BF16),
            pltpu.VMEM((PEERS * CAP, SUB, LANES), BF16),
            pltpu.VMEM((2048, 512), BF16),
            pltpu.VMEM((2048, 512), BF16),
            pltpu.VMEM((512, 2048), BF16),
            pltpu.VMEM((2048, 512), BF16),
            pltpu.VMEM((2048, 512), BF16),
            pltpu.VMEM((512, 2048), BF16),
            pltpu.VMEM((2, 8, 4, 4, 16, 256), BF16),
            pltpu.VMEM((128 * SUB, LANES), F32),
            pltpu.VMEM((128, 2048), BF16),
            dma((4,)), dma, pltpu.SemaphoreType.REGULAR, pltpu.SemaphoreType.REGULAR, dma,
            dma, dma((3,)), dma((3,)), dma((3,)), dma, dma((4,)), dma((4,)),
            dma, dma((GROUPS,)), dma, dma((GROUPS,)),
        ],
        compiler_params=pltpu.CompilerParams(
            collective_id=0, has_side_effects=True, vmem_limit_bytes=56 << 20
        ),
    )(
        routes.T, route_weights.T, tokens, norm_gain.reshape(1, -1),
        dense_gate.reshape(SUB, LANES), w_gate[0], w_up[0], w_down[0], dense_in, dense_out,
    )


def solution(mesh):
    placed = (
        P(("ep", "tp"), None),
        P(),
        P(("ep", "tp"), None),
        P(("ep", "tp"), None),
        P("ep", None, "tp"),
        P("ep", None, "tp"),
        P("ep", "tp", None),
        P("ep", None),
        P("ep", None),
        P(),
    )
    return jax.shard_map(
        shards, mesh=mesh, in_specs=placed, out_specs=P(("ep", "tp"), None), check_vma=False
    )
```

```python
import jax
import jax.numpy as jnp
from jax import lax
from jax.experimental import pallas as pl
from jax.experimental.pallas import tpu as pltpu
from jax.sharding import PartitionSpec as P

CLAMP_LIMIT = 7.0
SLOPE_ALPHA = 1.702
NORM_EPS = 1e-06
MESH = pl.DeviceIdType.MESH
BF16 = jnp.bfloat16
F32 = jnp.float32

PEERS = 128
CAP = 3
LANES = 128
SUB = 16
SELF = 7
GROUPS = 2
PER_GROUP = PEERS // GROUPS
ROWS = PER_GROUP * CAP
PACK = 16


def place_of(dz, dy, dx):
    j = jnp.where(dz == 0, 0, jnp.where(dz <= 4, 2 * dz - 1, 2 * (8 - dz)))
    return (dx * 4 + dy) * 8 + 7 - j


def offset_of(k):
    j = 7 - lax.rem(k, 8)
    odd = lax.rem(j, 2)
    half = lax.div(j, 2)
    dz = lax.rem(odd * (half + 1) + (1 - odd) * (8 - half), 8)
    r = lax.div(k, 8)
    return dz, lax.rem(r, 4), lax.div(r, 4)


def clamped_unit(gate_pre, up_pre):
    gate_clip = jnp.minimum(gate_pre, CLAMP_LIMIT)
    up_clip = jnp.clip(up_pre, -CLAMP_LIMIT, CLAMP_LIMIT)
    return ((up_clip + 1.0) * gate_clip * jax.nn.sigmoid(SLOPE_ALPHA * gate_clip)).astype(BF16)


def kernel(
    routes_hbm, rw_hbm, tok_hbm, gain_hbm, dgate_hbm, wg_hbm, wu_hbm, wd_hbm, din_hbm, dout_hbm,
    o_ref,
    routes, gain, dgate, table, index, rw,
    tok, x2, x3, send, recv, xg, hid, acc, outb, ret, wg, wu, wd, wgo, wuo, wdo, dense, branch,
    small_sem, index_sem, y_sem, x_sem,
    tok_sem, w_sem, wsend_sem, wrecv_sem, d_sem, dsend_sem, drecv_sem,
    send_sem, recv_sem, rsend_sem, rrecv_sem,
):
    me = lax.axis_index("ep")
    tp = lax.axis_index("tp")
    z, y, x = lax.div(me, 16), lax.rem(lax.div(me, 4), 4), lax.rem(me, 4)

    def chip(dz, dy, dx):
        return (
            lax.rem(z + dz, 8) * 16 + lax.rem(y + dy, 4) * 4 + lax.rem(x + dx, 4)
        )

    def back(dz, dy, dx):
        return (
            lax.rem(z + 8 - dz, 8) * 16 + lax.rem(y + 4 - dy, 4) * 4 + lax.rem(x + 4 - dx, 4)
        )

    small = [
        pltpu.make_async_copy(a, b, small_sem.at[i])
        for i, (a, b) in enumerate(
            ((routes_hbm, routes), (gain_hbm, gain), (rw_hbm, rw), (dgate_hbm, dgate))
        )
    ]
    tok_copy = pltpu.make_async_copy(tok_hbm, tok, tok_sem)
    small[0].start()
    tok_copy.start()

    def greet(sem, device):
        pl.semaphore_signal(sem, inc=1, device_id=device, device_id_type=MESH)

    barrier = pltpu.get_barrier_semaphore()
    for d in (4, 3, 5, 2, 6, 1, 7):
        greet(barrier, (chip(d, 0, 0), tp))
    for d in (2, 1, 3):
        greet(barrier, (chip(0, d, 0), tp))
        greet(barrier, (chip(0, 0, d), tp))
    greet(barrier, (me, 1 - tp))
    for copy in small[1:]:
        copy.start()

    @pl.when(tp == 0)
    def _():
        pltpu.make_async_copy(din_hbm, dense.at[0, z, y, x], d_sem).start()

    @pl.when(tp == 1)
    def _():
        pltpu.make_async_copy(dout_hbm, dense.at[1, z, y, x], d_sem).start()

    own = [
        pltpu.make_async_copy(a, b, w_sem.at[i])
        for i, (a, b) in enumerate(((wg_hbm, wg), (wu_hbm, wu), (wd_hbm, wd)))
    ]
    other = [
        pltpu.make_async_remote_copy(
            src_ref=a, dst_ref=b, send_sem=wsend_sem.at[i], recv_sem=wrecv_sem.at[i],
            device_id=(me, 1 - tp), device_id_type=MESH,
        )
        for i, (a, b) in enumerate(((wg_hbm, wgo), (wu_hbm, wuo), (wd_hbm, wdo)))
    ]

    table[...] = jnp.zeros_like(table)
    small[0].wait()
    tok_copy.wait()
    small[1].wait()
    chosen = routes[...]
    place = place_of(
        (lax.shift_right_logical(chosen, 4) - z) & 7,
        ((lax.shift_right_logical(chosen, 2) & 3) - y) & 3,
        ((chosen & 3) - x) & 3,
    )
    sub = lax.broadcasted_iota(jnp.int32, (PEERS, 128), 0)
    lane = lax.broadcasted_iota(jnp.int32, (PEERS, 128), 1)
    before = jnp.where(sub < lane, 1.0, 0.0).astype(BF16)
    token = lax.broadcasted_iota(jnp.int32, (8, 128), 1).astype(F32).astype(BF16)
    hits, slots = [], []
    for c in range(2):
        hit = jnp.where(sub == place[c : c + 1, :], 1.0, 0.0)
        earlier = jnp.dot(hit.astype(BF16), before, preferred_element_type=F32)
        if c == 1:
            earlier = earlier + jnp.sum(hits[0], axis=1, keepdims=True)
        slot = jnp.sum(hit * earlier, axis=0, keepdims=True)
        table[3 + c : 4 + c, :] = jnp.clip(
            place[c : c + 1, :] * CAP + slot.astype(jnp.int32), 0, PEERS * CAP - 1
        )
        hits.append(hit)
        slots.append(slot)
    for s in range(CAP):
        held = sum(jnp.where(slots[c] == s, hits[c], 0.0) for c in range(2)).astype(BF16)
        named = lax.dot_general(
            token, held, (((1,), (1,)), ((), ())), preferred_element_type=F32
        )
        table[s : s + 1, :] = jnp.clip(named[:1].astype(jnp.int32), 0, 127)
    index_copy = pltpu.make_async_copy(table, index, index_sem)
    index_copy.start()

    for i in range(8):
        rows = slice(i * 16, i * 16 + 16)
        wide = tok[rows, :].astype(F32)
        scale = lax.rsqrt(jnp.mean(wide * wide, axis=1, keepdims=True) + NORM_EPS)
        normed = (wide * scale * gain[...]).astype(BF16)
        x2[rows, :] = normed
        x3[rows] = normed.reshape(16, SUB, LANES)
    pl.semaphore_wait(barrier, 14)
    for d in (2, 1, 3):
        greet(y_sem, (chip(0, d, 0), tp))
    pltpu.make_async_copy(din_hbm, dense.at[tp, z, y, x], d_sem).wait()
    index_copy.wait()

    def spread(stage, count, block, target):
        for d in range(1, count):
            pltpu.make_async_remote_copy(
                src_ref=block, dst_ref=block, send_sem=dsend_sem.at[stage],
                recv_sem=drecv_sem.at[stage], device_id=(target(d), tp), device_id_type=MESH,
            ).start()

    def along_y(d):
        return chip(0, d, 0)

    def along_x(d):
        return chip(0, 0, d)

    z_all = dense.at[tp, pl.ds(0, 7), y, x]
    second_all = dense.at[tp, :, pl.ds(0, 3), x]
    third_all = dense.at[tp, :, :, pl.ds(0, 3)]

    def all_in(ref, sem):
        pltpu.make_async_copy(ref, ref, sem).wait()

    def pack(k, c):
        for s in range(CAP):
            send[k * CAP + s] = x3[index[s, k]]
        return c

    def dispatch(k, c):
        rows = pl.ds(k * CAP, CAP)

        @pl.when(k != SELF)
        def _():
            pltpu.make_async_remote_copy(
                src_ref=send.at[rows], dst_ref=recv.at[rows], send_sem=send_sem,
                recv_sem=recv_sem.at[lax.div(k, PER_GROUP)],
                device_id=(chip(*offset_of(k)), tp), device_id_type=MESH,
            ).start()

        return c

    lax.fori_loop(0, 16, pack, 0, unroll=4)
    lax.fori_loop(0, 8, dispatch, 0)
    spread(0, 8, dense.at[tp, z, y, x], lambda d: chip(d, 0, 0))
    lax.fori_loop(16, 32, pack, 0, unroll=4)
    pl.semaphore_wait(y_sem, 3)
    for d in (2, 1, 3):
        greet(x_sem, (chip(0, 0, d), tp))
    lax.fori_loop(8, 32, dispatch, 0)
    lax.fori_loop(32, 64, pack, 0, unroll=4)
    pl.semaphore_wait(x_sem, 3)
    lax.fori_loop(32, 64, dispatch, 0)
    for copy in own:
        copy.start()
    lax.fori_loop(64, 128, pack, 0, unroll=4)
    for s in range(CAP):
        recv[SELF * CAP + s] = send[SELF * CAP + s]

    all_in(z_all, drecv_sem.at[0])

    @pl.when(tp == 0)
    def _():
        spread(1, 4, dense.at[0, :, y, x], along_y)

    @pl.when(tp == 1)
    def _():
        spread(1, 4, dense.at[1, :, y, x], along_x)

    lax.fori_loop(64, 128, dispatch, 0)
    for copy in other:
        copy.start()
    all_in(second_all, drecv_sem.at[1])

    @pl.when(tp == 0)
    def _():
        spread(2, 4, dense.at[0, :, :, x], along_x)

    @pl.when(tp == 1)
    def _():
        spread(2, 4, dense.at[1, :, y], along_y)

    def answer(k, c):
        rows = pl.ds(k * CAP, CAP)

        @pl.when(k != SELF)
        def _():
            pltpu.make_async_remote_copy(
                src_ref=outb.at[rows], dst_ref=ret.at[rows], send_sem=rsend_sem,
                recv_sem=rrecv_sem.at[lax.div(k, PER_GROUP)],
                device_id=(back(*offset_of(k)), tp), device_id_type=MESH,
            ).start()

        return c

    def group_bytes(g):
        return PER_GROUP - 1 if g == 0 else PER_GROUP

    for g in range(GROUPS):
        base = g * ROWS
        all_in(recv.at[pl.ds(0, group_bytes(g) * CAP)], recv_sem.at[g])

        for r in range(0, ROWS, 16):
            xg[r : r + 16, :] = recv[base + r : base + r + 16].reshape(16, SUB * LANES)

        for h, (gate_w, up_w) in enumerate(((wg, wu), (wgo, wuo))):
            if g == 0:
                if h == 0:
                    for copy in own:
                        copy.wait()
                else:
                    for copy in other:
                        copy.wait_recv()
            for t in range(2):
                cols = slice(t * 256, t * 256 + 256)
                hid[:, h * 512 + t * 256 : h * 512 + t * 256 + 256] = clamped_unit(
                    jnp.dot(xg[...], gate_w[:, cols], preferred_element_type=F32),
                    jnp.dot(xg[...], up_w[:, cols], preferred_element_type=F32),
                )

        for t in range(8):
            cols = slice(t * 256, t * 256 + 256)
            first = jnp.dot(hid[:, :512], wd[:, cols], preferred_element_type=F32).astype(BF16)
            second = jnp.dot(hid[:, 512:], wdo[:, cols], preferred_element_type=F32).astype(BF16)
            summed = first.astype(F32) + second.astype(F32)
            for i in range(2):
                acc[pl.ds(2 * t + i, ROWS, stride=SUB), :] = summed[:, i * LANES : (i + 1) * LANES]

        for r in range(0, ROWS, 16):
            outb[base + r : base + r + 16] = (
                acc[r * SUB : (r + 16) * SUB, :].reshape(16, SUB, LANES).astype(BF16)
            )

        lax.fori_loop(g * PER_GROUP, (g + 1) * PER_GROUP, answer, 0)

    for s in range(CAP):
        ret[SELF * CAP + s] = outb[SELF * CAP + s]

    all_in(third_all, drecv_sem.at[2])
    swap = pltpu.make_async_remote_copy(
        src_ref=dense.at[tp], dst_ref=dense.at[tp], send_sem=dsend_sem.at[3],
        recv_sem=drecv_sem.at[3], device_id=(me, 1 - tp), device_id_type=MESH,
    )
    swap.start()
    swap.wait_recv()

    pre = jnp.zeros((128, 256), F32)
    for i in range(8):
        pre = pre + jnp.dot(
            x2[:, i * 256 : (i + 1) * 256], dense[0, i].reshape(256, 256), preferred_element_type=F32
        )
    dense_hidden = jax.nn.silu(pre).astype(BF16)
    small[3].wait()
    gate = jax.nn.sigmoid(dgate[...])
    for i in range(8):
        part = lax.dot_general(
            dense_hidden, dense[1, i].reshape(256, 256), (((1,), (1,)), ((), ())),
            preferred_element_type=F32,
        )
        for j in range(2):
            at = 2 * i + j
            branch[pl.ds(at, 128, stride=SUB), :] = (
                part[:, j * LANES : (j + 1) * LANES] * gate[at : at + 1, :]
            )

    small[2].wait()
    for g in range(GROUPS):
        all_in(ret.at[pl.ds(0, group_bytes(g) * CAP)], rrecv_sem.at[g])

    def combine(t, c):
        tile = pl.ds(pl.multiple_of(t * SUB, SUB), SUB)
        acc[tile, :] = (
            rw[0, t] * ret[index[3, t]].astype(F32) + rw[1, t] * ret[index[4, t]].astype(F32)
        ) + branch[tile, :]
        return c

    for r in range(0, 128, 16):
        lax.fori_loop(r, r + 16, combine, 0, unroll=8)
        o_ref[r : r + 16, :] = (
            acc[r * SUB : (r + 16) * SUB, :].reshape(16, SUB * LANES).astype(BF16)
        )

    all_in(send.at[pl.ds(0, (PEERS - 1) * CAP)], send_sem)
    all_in(outb.at[pl.ds(0, (PEERS - 1) * CAP)], rsend_sem)
    for copy in other:
        copy.wait_send()
    all_in(z_all, dsend_sem.at[0])
    all_in(second_all, dsend_sem.at[1])
    all_in(third_all, dsend_sem.at[2])
    swap.wait_send()


def shards(
    tokens, norm_gain, routes, route_weights, w_gate, w_up, w_down, dense_in, dense_out, dense_gate
):
    hbm = pl.BlockSpec(memory_space=pl.ANY)
    dma = pltpu.SemaphoreType.DMA
    return pl.pallas_call(
        kernel,
        out_shape=jax.ShapeDtypeStruct((128, 2048), BF16),
        in_specs=[hbm] * 10,
        out_specs=pl.BlockSpec(memory_space=pltpu.VMEM),
        scratch_shapes=[
            pltpu.VMEM((2, 128), jnp.int32),
            pltpu.VMEM((1, 2048), F32),
            pltpu.VMEM((SUB, LANES), F32),
            pltpu.VMEM((8, 128), jnp.int32),
            pltpu.SMEM((8, 128), jnp.int32),
            pltpu.SMEM((2, 128), F32),
            pltpu.VMEM((128, 2048), BF16),
            pltpu.VMEM((128, 2048), BF16),
            pltpu.VMEM((128, SUB, LANES), BF16),
            pltpu.VMEM((PEERS * CAP, SUB, LANES), BF16),
            pltpu.VMEM((PEERS * CAP, SUB, LANES), BF16),
            pltpu.VMEM((ROWS, 2048), BF16),
            pltpu.VMEM((ROWS, 1024), BF16),
            pltpu.VMEM((ROWS * SUB, LANES), F32),
            pltpu.VMEM((PEERS * CAP, SUB, LANES), BF16),
            pltpu.VMEM((PEERS * CAP, SUB, LANES), BF16),
            pltpu.VMEM((2048, 512), BF16),
            pltpu.VMEM((2048, 512), BF16),
            pltpu.VMEM((512, 2048), BF16),
            pltpu.VMEM((2048, 512), BF16),
            pltpu.VMEM((2048, 512), BF16),
            pltpu.VMEM((512, 2048), BF16),
            pltpu.VMEM((2, 8, 4, 4, 16, 256), BF16),
            pltpu.VMEM((128 * SUB, LANES), F32),
            dma((4,)), dma, pltpu.SemaphoreType.REGULAR, pltpu.SemaphoreType.REGULAR,
            dma, dma((3,)), dma((3,)), dma((3,)), dma, dma((4,)), dma((4,)),
            dma, dma((GROUPS,)), dma, dma((GROUPS,)),
        ],
        compiler_params=pltpu.CompilerParams(
            collective_id=0, has_side_effects=True, vmem_limit_bytes=50 << 20
        ),
    )(
        *(
            pltpu.with_memory_space_constraint(operand, pltpu.HBM)
            for operand in (
                routes.T, route_weights.T, tokens, norm_gain.reshape(1, -1),
                dense_gate.reshape(SUB, LANES), w_gate[0], w_up[0], w_down[0], dense_in, dense_out,
            )
        )
    )


def solution(mesh):
    placed = (
        P(("ep", "tp"), None),
        P(),
        P(("ep", "tp"), None),
        P(("ep", "tp"), None),
        P("ep", None, "tp"),
        P("ep", None, "tp"),
        P("ep", "tp", None),
        P("ep", None),
        P("ep", None),
        P(),
    )
    return jax.shard_map(
        shards, mesh=mesh, in_specs=placed, out_specs=P(("ep", "tp"), None), check_vma=False
    )
```

```python
import jax
import jax.numpy as jnp
from jax import lax
from jax.experimental import pallas as pl
from jax.experimental.pallas import tpu as pltpu
from jax.sharding import PartitionSpec as P

CLAMP_LIMIT = 7.0
SLOPE_ALPHA = 1.702
NORM_EPS = 1e-06
MESH = pl.DeviceIdType.MESH
BF16 = jnp.bfloat16
F32 = jnp.float32

PEERS = 128
CAP = 3
LANES = 128
SUB = 16
SELF = 7
GROUPS = 2
PER_GROUP = PEERS // GROUPS
ROWS = PER_GROUP * CAP
LOCAL = 3
DZ = (4, 5, 3, 6, 2, 7, 1, 0)


def place_of(dz, dy, dx):
    j = jnp.where(dz == 0, 0, jnp.where(dz <= 4, 2 * dz - 1, 2 * (8 - dz)))
    return (dx * 4 + dy) * 8 + 7 - j


def offset_of(k):
    j = 7 - lax.rem(k, 8)
    odd = lax.rem(j, 2)
    half = lax.div(j, 2)
    dz = lax.rem(odd * (half + 1) + (1 - odd) * (8 - half), 8)
    r = lax.div(k, 8)
    return dz, lax.rem(r, 4), lax.div(r, 4)


def clamped_unit(gate_pre, up_pre):
    gate_clip = jnp.minimum(gate_pre, CLAMP_LIMIT)
    up_clip = jnp.clip(up_pre, -CLAMP_LIMIT, CLAMP_LIMIT)
    return ((up_clip + 1.0) * gate_clip * jax.nn.sigmoid(SLOPE_ALPHA * gate_clip)).astype(BF16)


def kernel(
    routes_hbm, rw_hbm, tok_hbm, gain_hbm, dgate_hbm, wg_hbm, wu_hbm, wd_hbm, din_hbm, dout_hbm,
    o_ref,
    routes, gain, dgate, table, index, rw, xn, tn, indexn,
    tok, x2, x3, send, recv, xg, hid, acc, outb, ret, wg, wu, wd, wgo, wuo, wdo, dense, branch,
    small_sem, index_sem, y_sem, x_sem, nsend_sem, nrecv_sem, tsend_sem, trecv_sem, indexn_sem,
    tok_sem, w_sem, wsend_sem, wrecv_sem, d_sem, dsend_sem, drecv_sem,
    send_sem, recv_sem, rsend_sem, rrecv_sem,
):
    me = lax.axis_index("ep")
    tp = lax.axis_index("tp")
    z, y, x = lax.div(me, 16), lax.rem(lax.div(me, 4), 4), lax.rem(me, 4)

    def chip(dz, dy, dx):
        return (
            lax.rem(z + dz, 8) * 16 + lax.rem(y + dy, 4) * 4 + lax.rem(x + dx, 4)
        )

    def back(dz, dy, dx):
        return (
            lax.rem(z + 8 - dz, 8) * 16 + lax.rem(y + 4 - dy, 4) * 4 + lax.rem(x + 4 - dx, 4)
        )

    small = [
        pltpu.make_async_copy(a, b, small_sem.at[i])
        for i, (a, b) in enumerate(
            ((routes_hbm, routes), (gain_hbm, gain), (rw_hbm, rw), (dgate_hbm, dgate))
        )
    ]
    tok_copy = pltpu.make_async_copy(tok_hbm, tok, tok_sem)
    small[0].start()
    tok_copy.start()

    def greet(sem, device):
        pl.semaphore_signal(sem, inc=1, device_id=device, device_id_type=MESH)

    barrier = pltpu.get_barrier_semaphore()
    for d in (4, 3, 5, 2, 6, 1, 7):
        greet(barrier, (chip(d, 0, 0), tp))
    for d in (2, 1, 3):
        greet(barrier, (chip(0, d, 0), tp))
        greet(barrier, (chip(0, 0, d), tp))
    greet(barrier, (me, 1 - tp))
    for copy in small[1:]:
        copy.start()

    @pl.when(tp == 0)
    def _():
        pltpu.make_async_copy(din_hbm, dense.at[0, z, y, x], d_sem).start()

    @pl.when(tp == 1)
    def _():
        pltpu.make_async_copy(dout_hbm, dense.at[1, z, y, x], d_sem).start()

    own = [
        pltpu.make_async_copy(a, b, w_sem.at[i])
        for i, (a, b) in enumerate(((wg_hbm, wg), (wu_hbm, wu), (wd_hbm, wd)))
    ]
    other = [
        pltpu.make_async_remote_copy(
            src_ref=a, dst_ref=b, send_sem=wsend_sem.at[i], recv_sem=wrecv_sem.at[i],
            device_id=(me, 1 - tp), device_id_type=MESH,
        )
        for i, (a, b) in enumerate(((wg_hbm, wgo), (wu_hbm, wuo), (wd_hbm, wdo)))
    ]

    table[...] = jnp.zeros_like(table)
    small[0].wait()
    tok_copy.wait()
    small[1].wait()
    chosen = routes[...]
    place = place_of(
        (lax.shift_right_logical(chosen, 4) - z) & 7,
        ((lax.shift_right_logical(chosen, 2) & 3) - y) & 3,
        ((chosen & 3) - x) & 3,
    )
    sub = lax.broadcasted_iota(jnp.int32, (PEERS, 128), 0)
    lane = lax.broadcasted_iota(jnp.int32, (PEERS, 128), 1)
    before = jnp.where(sub < lane, 1.0, 0.0).astype(BF16)
    token = lax.broadcasted_iota(jnp.int32, (8, 128), 1).astype(F32).astype(BF16)
    hits, slots = [], []
    for c in range(2):
        hit = jnp.where(sub == place[c : c + 1, :], 1.0, 0.0)
        earlier = jnp.dot(hit.astype(BF16), before, preferred_element_type=F32)
        if c == 1:
            earlier = earlier + jnp.sum(hits[0], axis=1, keepdims=True)
        slot = jnp.sum(hit * earlier, axis=0, keepdims=True)
        table[3 + c : 4 + c, :] = jnp.clip(
            place[c : c + 1, :] * CAP + slot.astype(jnp.int32), 0, PEERS * CAP - 1
        )
        hits.append(hit)
        slots.append(slot)
    for s in range(CAP):
        held = sum(jnp.where(slots[c] == s, hits[c], 0.0) for c in range(2)).astype(BF16)
        named = lax.dot_general(
            token, held, (((1,), (1,)), ((), ())), preferred_element_type=F32
        )
        table[s : s + 1, :] = jnp.clip(named[:1].astype(jnp.int32), 0, 127)
    index_copy = pltpu.make_async_copy(table, index, index_sem)
    index_copy.start()

    for i in range(8):
        rows = slice(i * 16, i * 16 + 16)
        wide = tok[rows, :].astype(F32)
        scale = lax.rsqrt(jnp.mean(wide * wide, axis=1, keepdims=True) + NORM_EPS)
        normed = (wide * scale * gain[...]).astype(BF16)
        x2[rows, :] = normed
        x3[rows] = normed.reshape(16, SUB, LANES)
    pl.semaphore_wait(barrier, 14)
    ahead = [
        pltpu.make_async_remote_copy(
            src_ref=a, dst_ref=b.at[i], send_sem=ss.at[i], recv_sem=rs.at[i],
            device_id=(chip(d, 0, 0), tp), device_id_type=MESH,
        )
        for a, b, ss, rs in (
            (table, tn, tsend_sem, trecv_sem), (x3, xn, nsend_sem, nrecv_sem)
        )
        for i, d in enumerate((1, 7))
    ]
    for copy in ahead:
        copy.start()
    for d in (2, 1, 3):
        greet(y_sem, (chip(0, d, 0), tp))
    pltpu.make_async_copy(din_hbm, dense.at[tp, z, y, x], d_sem).wait()
    index_copy.wait()

    def spread(stage, count, block, target):
        for d in range(1, count):
            pltpu.make_async_remote_copy(
                src_ref=block, dst_ref=block, send_sem=dsend_sem.at[stage],
                recv_sem=drecv_sem.at[stage], device_id=(target(d), tp), device_id_type=MESH,
            ).start()

    def along_y(d):
        return chip(0, d, 0)

    def along_x(d):
        return chip(0, 0, d)

    z_all = dense.at[tp, pl.ds(0, 7), y, x]
    second_all = dense.at[tp, :, pl.ds(0, 3), x]
    third_all = dense.at[tp, :, :, pl.ds(0, 3)]

    def all_in(ref, sem):
        pltpu.make_async_copy(ref, ref, sem).wait()

    def pack(k, rows_of, index_of):
        for s in range(CAP):
            send[k * CAP + s] = rows_of[index_of[s, k]]

    def dispatch(k, z_to, r):
        rows = pl.ds(k * CAP, CAP)
        device = z_to * 16 + lax.rem(y + lax.rem(r, 4), 4) * 4 + lax.rem(x + lax.div(r, 4), 4)
        pltpu.make_async_remote_copy(
            src_ref=send.at[rows], dst_ref=recv.at[rows], send_sem=send_sem,
            recv_sem=recv_sem.at[lax.div(k, PER_GROUP)],
            device_id=(device, tp), device_id_type=MESH,
        ).start()

    for r in range(4):
        pack(r * 8, x3, index)
    spread(0, 8, dense.at[tp, z, y, x], lambda d: chip(d, 0, 0))
    pl.semaphore_wait(y_sem, 3)
    for d in (2, 1, 3):
        greet(x_sem, (chip(0, 0, d), tp))
    for r in range(4):
        dispatch(r * 8, lax.rem(z + 4, 8), r)

    def pack_flat(r, c):
        pack(r * 8 + 7, x3, index)
        return c

    def dispatch_flat(r, c):
        dispatch(r * 8 + 7, z, r)
        return c

    lax.fori_loop(0, 16, pack_flat, 0)
    pl.semaphore_wait(x_sem, 3)
    lax.fori_loop(1, 16, dispatch_flat, 0)
    for copy in own:
        copy.start()
    for copy in other:
        copy.start()

    onward = []
    for i in range(2):
        ahead[i].wait_recv()
        onward.append(pltpu.make_async_copy(tn.at[i], indexn.at[i], indexn_sem.at[i]))
        onward[i].start()
    for i in range(2):
        onward[i].wait()
    for i in range(2):
        ahead[2 + i].wait_recv()

    def relay_pair(h, c):
        def each(visit):
            for p in range(2):
                r = 2 * h + p
                for at in range(7):
                    if at == 0:
                        pl.when(h >= 2)(lambda r=r, p=p: visit(r, 0, p, False))
                    else:
                        visit(r, at, at % 2, p == 0 and at >= 5)

        def do_pack(r, at, i, local):
            pack(r * 8 + at, xn.at[i], indexn.at[i])

        def do_send(r, at, i, local):
            z_to = lax.rem(z + (7 if i == 0 else 1) + DZ[at], 8)
            if local:
                pl.when(h > 0)(lambda: dispatch(r * 8 + at, z_to, r))
            else:
                dispatch(r * 8 + at, z_to, r)

        each(do_pack)
        each(do_send)
        return c

    lax.fori_loop(0, 4, relay_pair, 0)
    for s in range(LOCAL * CAP):
        recv[5 * CAP + s] = send[5 * CAP + s]

    all_in(z_all, drecv_sem.at[0])

    @pl.when(tp == 0)
    def _():
        spread(1, 4, dense.at[0, :, y, x], along_y)

    @pl.when(tp == 1)
    def _():
        spread(1, 4, dense.at[1, :, y, x], along_x)

    lax.fori_loop(4, 8, relay_pair, 0)
    all_in(second_all, drecv_sem.at[1])

    @pl.when(tp == 0)
    def _():
        spread(2, 4, dense.at[0, :, :, x], along_x)

    @pl.when(tp == 1)
    def _():
        spread(2, 4, dense.at[1, :, y], along_y)

    def answer(k, c):
        rows = pl.ds(k * CAP, CAP)

        @pl.when(k != SELF)
        def _():
            pltpu.make_async_remote_copy(
                src_ref=outb.at[rows], dst_ref=ret.at[rows], send_sem=rsend_sem,
                recv_sem=rrecv_sem.at[lax.div(k, PER_GROUP)],
                device_id=(back(*offset_of(k)), tp), device_id_type=MESH,
            ).start()

        return c

    def group_bytes(g):
        return PER_GROUP - 1 if g == 0 else PER_GROUP

    for g in range(GROUPS):
        base = g * ROWS
        all_in(recv.at[pl.ds(0, (PER_GROUP - LOCAL * (g == 0)) * CAP)], recv_sem.at[g])

        for r in range(0, ROWS, 16):
            xg[r : r + 16, :] = recv[base + r : base + r + 16].reshape(16, SUB * LANES)

        for h, (gate_w, up_w) in enumerate(((wg, wu), (wgo, wuo))):
            if g == 0:
                if h == 0:
                    for copy in own:
                        copy.wait()
                else:
                    for copy in other:
                        copy.wait_recv()
            for t in range(2):
                cols = slice(t * 256, t * 256 + 256)
                hid[:, h * 512 + t * 256 : h * 512 + t * 256 + 256] = clamped_unit(
                    jnp.dot(xg[...], gate_w[:, cols], preferred_element_type=F32),
                    jnp.dot(xg[...], up_w[:, cols], preferred_element_type=F32),
                )

        for t in range(8):
            cols = slice(t * 256, t * 256 + 256)
            first = jnp.dot(hid[:, :512], wd[:, cols], preferred_element_type=F32).astype(BF16)
            second = jnp.dot(hid[:, 512:], wdo[:, cols], preferred_element_type=F32).astype(BF16)
            summed = first.astype(F32) + second.astype(F32)
            for i in range(2):
                acc[pl.ds(2 * t + i, ROWS, stride=SUB), :] = summed[:, i * LANES : (i + 1) * LANES]

        for r in range(0, ROWS, 16):
            outb[base + r : base + r + 16] = (
                acc[r * SUB : (r + 16) * SUB, :].reshape(16, SUB, LANES).astype(BF16)
            )

        lax.fori_loop(g * PER_GROUP, (g + 1) * PER_GROUP, answer, 0)

    for s in range(CAP):
        ret[SELF * CAP + s] = outb[SELF * CAP + s]

    all_in(third_all, drecv_sem.at[2])
    swap = pltpu.make_async_remote_copy(
        src_ref=dense.at[tp], dst_ref=dense.at[tp], send_sem=dsend_sem.at[3],
        recv_sem=drecv_sem.at[3], device_id=(me, 1 - tp), device_id_type=MESH,
    )
    swap.start()
    swap.wait_recv()

    pre = jnp.zeros((128, 256), F32)
    for i in range(8):
        pre = pre + jnp.dot(
            x2[:, i * 256 : (i + 1) * 256], dense[0, i].reshape(256, 256), preferred_element_type=F32
        )
    dense_hidden = jax.nn.silu(pre).astype(BF16)
    small[3].wait()
    gate = jax.nn.sigmoid(dgate[...])
    for i in range(8):
        part = lax.dot_general(
            dense_hidden, dense[1, i].reshape(256, 256), (((1,), (1,)), ((), ())),
            preferred_element_type=F32,
        )
        for j in range(2):
            at = 2 * i + j
            branch[pl.ds(at, 128, stride=SUB), :] = (
                part[:, j * LANES : (j + 1) * LANES] * gate[at : at + 1, :]
            )

    small[2].wait()
    for g in range(GROUPS):
        all_in(ret.at[pl.ds(0, group_bytes(g) * CAP)], rrecv_sem.at[g])

    def combine(t, c):
        tile = pl.ds(pl.multiple_of(t * SUB, SUB), SUB)
        acc[tile, :] = (
            rw[0, t] * ret[index[3, t]].astype(F32) + rw[1, t] * ret[index[4, t]].astype(F32)
        ) + branch[tile, :]
        return c

    for r in range(0, 128, 16):
        lax.fori_loop(r, r + 16, combine, 0, unroll=8)
        o_ref[r : r + 16, :] = (
            acc[r * SUB : (r + 16) * SUB, :].reshape(16, SUB * LANES).astype(BF16)
        )

    all_in(send.at[pl.ds(0, (PEERS - LOCAL) * CAP)], send_sem)
    for copy in ahead:
        copy.wait_send()
    all_in(outb.at[pl.ds(0, (PEERS - 1) * CAP)], rsend_sem)
    for copy in other:
        copy.wait_send()
    all_in(z_all, dsend_sem.at[0])
    all_in(second_all, dsend_sem.at[1])
    all_in(third_all, dsend_sem.at[2])
    swap.wait_send()


def shards(
    tokens, norm_gain, routes, route_weights, w_gate, w_up, w_down, dense_in, dense_out, dense_gate
):
    hbm = pl.BlockSpec(memory_space=pl.ANY)
    dma = pltpu.SemaphoreType.DMA
    return pl.pallas_call(
        kernel,
        out_shape=jax.ShapeDtypeStruct((128, 2048), BF16),
        in_specs=[hbm] * 10,
        out_specs=pl.BlockSpec(memory_space=pltpu.VMEM),
        scratch_shapes=[
            pltpu.VMEM((2, 128), jnp.int32),
            pltpu.VMEM((1, 2048), F32),
            pltpu.VMEM((SUB, LANES), F32),
            pltpu.VMEM((8, 128), jnp.int32),
            pltpu.SMEM((8, 128), jnp.int32),
            pltpu.SMEM((2, 128), F32),
            pltpu.VMEM((2, 128, SUB, LANES), BF16),
            pltpu.VMEM((2, 8, 128), jnp.int32),
            pltpu.SMEM((2, 8, 128), jnp.int32),
            pltpu.VMEM((128, 2048), BF16),
            pltpu.VMEM((128, 2048), BF16),
            pltpu.VMEM((128, SUB, LANES), BF16),
            pltpu.VMEM((PEERS * CAP, SUB, LANES), BF16),
            pltpu.VMEM((PEERS * CAP, SUB, LANES), BF16),
            pltpu.VMEM((ROWS, 2048), BF16),
            pltpu.VMEM((ROWS, 1024), BF16),
            pltpu.VMEM((ROWS * SUB, LANES), F32),
            pltpu.VMEM((PEERS * CAP, SUB, LANES), BF16),
            pltpu.VMEM((PEERS * CAP, SUB, LANES), BF16),
            pltpu.VMEM((2048, 512), BF16),
            pltpu.VMEM((2048, 512), BF16),
            pltpu.VMEM((512, 2048), BF16),
            pltpu.VMEM((2048, 512), BF16),
            pltpu.VMEM((2048, 512), BF16),
            pltpu.VMEM((512, 2048), BF16),
            pltpu.VMEM((2, 8, 4, 4, 16, 256), BF16),
            pltpu.VMEM((128 * SUB, LANES), F32),
            dma((4,)), dma, pltpu.SemaphoreType.REGULAR, pltpu.SemaphoreType.REGULAR,
            dma((2,)), dma((2,)), dma((2,)), dma((2,)), dma((2,)),
            dma, dma((3,)), dma((3,)), dma((3,)), dma, dma((4,)), dma((4,)),
            dma, dma((GROUPS,)), dma, dma((GROUPS,)),
        ],
        compiler_params=pltpu.CompilerParams(
            collective_id=0, has_side_effects=True, vmem_limit_bytes=50 << 20
        ),
    )(
        *(
            pltpu.with_memory_space_constraint(operand, pltpu.HBM)
            for operand in (
                routes.T, route_weights.T, tokens, norm_gain.reshape(1, -1),
                dense_gate.reshape(SUB, LANES), w_gate[0], w_up[0], w_down[0], dense_in, dense_out,
            )
        )
    )


def solution(mesh):
    placed = (
        P(("ep", "tp"), None),
        P(),
        P(("ep", "tp"), None),
        P(("ep", "tp"), None),
        P("ep", None, "tp"),
        P("ep", None, "tp"),
        P("ep", "tp", None),
        P("ep", None),
        P("ep", None),
        P(),
    )
    return jax.shard_map(
        shards, mesh=mesh, in_specs=placed, out_specs=P(("ep", "tp"), None), check_vma=False
    )
```

```python
import jax
import jax.numpy as jnp
from jax import lax
from jax.experimental import pallas as pl
from jax.experimental.pallas import tpu as pltpu
from jax.sharding import PartitionSpec as P

CLAMP_LIMIT = 7.0
SLOPE_ALPHA = 1.702
NORM_EPS = 1e-06
MESH = pl.DeviceIdType.MESH
BF16 = jnp.bfloat16
F32 = jnp.float32

PEERS = 128
CAP = 3
LANES = 128
SUB = 16
SELF = 7
GROUPS = 4
PER_GROUP = PEERS // GROUPS
ROWS = PER_GROUP * CAP
LOCAL = 3
CHUNK = 16
DZ = (4, 5, 3, 6, 2, 7, 1, 0)


def place_of(dz, dy, dx):
    j = jnp.where(dz == 0, 0, jnp.where(dz <= 4, 2 * dz - 1, 2 * (8 - dz)))
    return (dx * 4 + dy) * 8 + 7 - j


def offset_of(k):
    j = 7 - lax.rem(k, 8)
    odd = lax.rem(j, 2)
    half = lax.div(j, 2)
    dz = lax.rem(odd * (half + 1) + (1 - odd) * (8 - half), 8)
    r = lax.div(k, 8)
    return dz, lax.rem(r, 4), lax.div(r, 4)


def clamped_unit(gate_pre, up_pre):
    gate_clip = jnp.minimum(gate_pre, CLAMP_LIMIT)
    up_clip = jnp.clip(up_pre, -CLAMP_LIMIT, CLAMP_LIMIT)
    return ((up_clip + 1.0) * gate_clip * jax.nn.sigmoid(SLOPE_ALPHA * gate_clip)).astype(BF16)


def kernel(
    routes_hbm, rw_hbm, tok_hbm, gain_hbm, dgate_hbm, wg_hbm, wu_hbm, wd_hbm, din_hbm, dout_hbm,
    o_ref,
    routes, gain, dgate, table, index, rw, xn, tn, indexn, share, sharen, part, pn, weight, weightn,
    tok, x2, x3, send, recv, xg, hid, acc, outb, ret, wg, wu, wd, wgo, wuo, wdo, dense, branch,
    small_sem, index_sem, y_sem, x_sem, nsend_sem, nrecv_sem, tsend_sem, trecv_sem, indexn_sem, ssend_sem, srecv_sem, weight_sem, weightn_sem, psend_sem, precv_sem,
    tok_sem, w_sem, wsend_sem, wrecv_sem, d_sem, dsend_sem, drecv_sem,
    send_sem, recv_sem, rsend_sem, rrecv_sem,
):
    me = lax.axis_index("ep")
    tp = lax.axis_index("tp")
    z, y, x = lax.div(me, 16), lax.rem(lax.div(me, 4), 4), lax.rem(me, 4)

    def chip(dz, dy, dx):
        return (
            lax.rem(z + dz, 8) * 16 + lax.rem(y + dy, 4) * 4 + lax.rem(x + dx, 4)
        )

    def back(dz, dy, dx):
        return (
            lax.rem(z + 8 - dz, 8) * 16 + lax.rem(y + 4 - dy, 4) * 4 + lax.rem(x + 4 - dx, 4)
        )

    small = [
        pltpu.make_async_copy(a, b, small_sem.at[i])
        for i, (a, b) in enumerate(
            ((routes_hbm, routes), (gain_hbm, gain), (rw_hbm, rw), (dgate_hbm, dgate))
        )
    ]
    tok_copy = pltpu.make_async_copy(tok_hbm, tok, tok_sem)
    small[0].start()
    tok_copy.start()

    def greet(sem, device):
        pl.semaphore_signal(sem, inc=1, device_id=device, device_id_type=MESH)

    barrier = pltpu.get_barrier_semaphore()
    for d in (4, 3, 5, 2, 6, 1, 7):
        greet(barrier, (chip(d, 0, 0), tp))
    for d in (2, 1, 3):
        greet(barrier, (chip(0, d, 0), tp))
        greet(barrier, (chip(0, 0, d), tp))
    greet(barrier, (me, 1 - tp))
    for copy in small[1:]:
        copy.start()

    @pl.when(tp == 0)
    def _():
        pltpu.make_async_copy(din_hbm, dense.at[0, z, y, x], d_sem).start()

    @pl.when(tp == 1)
    def _():
        pltpu.make_async_copy(dout_hbm, dense.at[1, z, y, x], d_sem).start()

    own = [
        pltpu.make_async_copy(a, b, w_sem.at[i])
        for i, (a, b) in enumerate(((wg_hbm, wg), (wu_hbm, wu), (wd_hbm, wd)))
    ]
    other = [
        pltpu.make_async_remote_copy(
            src_ref=a, dst_ref=b, send_sem=wsend_sem.at[i], recv_sem=wrecv_sem.at[i],
            device_id=(me, 1 - tp), device_id_type=MESH,
        )
        for i, (a, b) in enumerate(((wg_hbm, wgo), (wu_hbm, wuo), (wd_hbm, wdo)))
    ]

    table[...] = jnp.zeros_like(table)
    small[0].wait()
    tok_copy.wait()
    small[1].wait()
    chosen = routes[...]
    place = place_of(
        (lax.shift_right_logical(chosen, 4) - z) & 7,
        ((lax.shift_right_logical(chosen, 2) & 3) - y) & 3,
        ((chosen & 3) - x) & 3,
    )
    sub = lax.broadcasted_iota(jnp.int32, (PEERS, 128), 0)
    lane = lax.broadcasted_iota(jnp.int32, (PEERS, 128), 1)
    before = jnp.where(sub < lane, 1.0, 0.0).astype(BF16)
    token = lax.broadcasted_iota(jnp.int32, (8, 128), 1).astype(F32).astype(BF16)
    hits, slots = [], []
    for c in range(2):
        hit = jnp.where(sub == place[c : c + 1, :], 1.0, 0.0)
        earlier = jnp.dot(hit.astype(BF16), before, preferred_element_type=F32)
        if c == 1:
            earlier = earlier + jnp.sum(hits[0], axis=1, keepdims=True)
        slot = jnp.sum(hit * earlier, axis=0, keepdims=True)
        table[3 + c : 4 + c, :] = jnp.clip(
            place[c : c + 1, :] * CAP + slot.astype(jnp.int32), 0, PEERS * CAP - 1
        )
        hits.append(hit)
        slots.append(slot)
    for s in range(CAP):
        held = sum(jnp.where(slots[c] == s, hits[c], 0.0) for c in range(2)).astype(BF16)
        named = lax.dot_general(
            token, held, (((1,), (1,)), ((), ())), preferred_element_type=F32
        )
        table[s : s + 1, :] = jnp.clip(named[:1].astype(jnp.int32), 0, 127)
    index_copy = pltpu.make_async_copy(table, index, index_sem)
    index_copy.start()

    small[2].wait()
    at = place & 7
    flank = (at == 0) & (place >= 32)
    even = (lax.shift_right_logical(place, 3) & 1) == 0
    up = ((at == 2) | (at == 4) | (at == 6)) | (flank & even)
    down = ((at == 1) | (at == 3) | (at == 5)) | (flank & ~even)
    share[...] = jnp.zeros_like(share)
    share[0:2, :] = jnp.where(up, rw[...], 0.0)
    share[2:4, :] = jnp.where(down, rw[...], 0.0)
    share[4:6, :] = jnp.where(up | down, 0.0, rw[...])
    weight_copy = pltpu.make_async_copy(share, weight, weight_sem)
    weight_copy.start()

    for i in range(8):
        rows = slice(i * 16, i * 16 + 16)
        wide = tok[rows, :].astype(F32)
        scale = lax.rsqrt(jnp.mean(wide * wide, axis=1, keepdims=True) + NORM_EPS)
        normed = (wide * scale * gain[...]).astype(BF16)
        x2[rows, :] = normed
        x3[rows] = normed.reshape(16, SUB, LANES)
    def spread(stage, count, block, target):
        for d in range(1, count):
            pltpu.make_async_remote_copy(
                src_ref=block, dst_ref=block, send_sem=dsend_sem.at[stage],
                recv_sem=drecv_sem.at[stage], device_id=(target(d), tp), device_id_type=MESH,
            ).start()

    def along_y(d):
        return chip(0, d, 0)

    def along_x(d):
        return chip(0, 0, d)

    z_all = dense.at[tp, pl.ds(0, 7), y, x]
    second_all = dense.at[tp, :, pl.ds(0, 3), x]
    third_all = dense.at[tp, :, :, pl.ds(0, 3)]

    def all_in(ref, sem):
        pltpu.make_async_copy(ref, ref, sem).wait()

    pltpu.make_async_copy(din_hbm, dense.at[tp, z, y, x], d_sem).wait()
    pl.semaphore_wait(barrier, 14)
    spread(0, 8, dense.at[tp, z, y, x], lambda d: chip(d, 0, 0))
    ahead = [
        pltpu.make_async_remote_copy(
            src_ref=a, dst_ref=b.at[i], send_sem=ss.at[i], recv_sem=rs.at[i],
            device_id=(chip(d, 0, 0), tp), device_id_type=MESH,
        )
        for a, b, ss, rs in (
            (table, tn, tsend_sem, trecv_sem), (x3, xn, nsend_sem, nrecv_sem),
            (share, sharen, ssend_sem, srecv_sem),
        )
        for i, d in enumerate((1, 7))
    ]
    for copy in ahead:
        copy.start()
    for d in (2, 1, 3):
        greet(y_sem, (chip(0, d, 0), tp))
    index_copy.wait()

    def pack(k, rows_of, index_of):
        for s in range(CAP):
            send[k * CAP + s] = rows_of[index_of[s, k]]

    def dispatch(k, z_to, r):
        rows = pl.ds(k * CAP, CAP)
        device = z_to * 16 + lax.rem(y + lax.rem(r, 4), 4) * 4 + lax.rem(x + lax.div(r, 4), 4)
        pltpu.make_async_remote_copy(
            src_ref=send.at[rows], dst_ref=recv.at[rows], send_sem=send_sem,
            recv_sem=recv_sem.at[lax.div(k, PER_GROUP)],
            device_id=(device, tp), device_id_type=MESH,
        ).start()

    for r in range(4):
        pack(r * 8, x3, index)
    pl.semaphore_wait(y_sem, 3)
    for d in (2, 1, 3):
        greet(x_sem, (chip(0, 0, d), tp))
    for r in range(4):
        dispatch(r * 8, lax.rem(z + 4, 8), r)

    def pack_flat(r, c):
        pack(r * 8 + 7, x3, index)
        return c

    def dispatch_flat(r, c):
        dispatch(r * 8 + 7, z, r)
        return c

    lax.fori_loop(0, 16, pack_flat, 0)
    pl.semaphore_wait(x_sem, 3)
    lax.fori_loop(1, 16, dispatch_flat, 0)
    for copy in own:
        copy.start()
    for copy in other:
        copy.start()

    all_in(z_all, drecv_sem.at[0])

    @pl.when(tp == 0)
    def _():
        spread(1, 4, dense.at[0, :, y, x], along_y)

    @pl.when(tp == 1)
    def _():
        spread(1, 4, dense.at[1, :, y, x], along_x)

    all_in(second_all, drecv_sem.at[1])

    @pl.when(tp == 0)
    def _():
        spread(2, 4, dense.at[0, :, :, x], along_x)

    @pl.when(tp == 1)
    def _():
        spread(2, 4, dense.at[1, :, y], along_y)

    onward = []
    for i in range(2):
        ahead[i].wait_recv()
        onward.append(pltpu.make_async_copy(tn.at[i], indexn.at[i], indexn_sem.at[i]))
        onward[i].start()
    for i in range(2):
        onward[i].wait()
    for i in range(2):
        ahead[2 + i].wait_recv()

    def relay_pair(h, c):
        def each(visit):
            for p in range(2):
                r = 2 * h + p
                for at in range(7):
                    if at == 0:
                        pl.when(h >= 2)(lambda r=r, p=p: visit(r, 0, p, False))
                    else:
                        visit(r, at, at % 2, p == 0 and at >= 5)

        def do_pack(r, at, i, local):
            pack(r * 8 + at, xn.at[i], indexn.at[i])

        def do_send(r, at, i, local):
            z_to = lax.rem(z + (7 if i == 0 else 1) + DZ[at], 8)
            if local:
                pl.when(h > 0)(lambda: dispatch(r * 8 + at, z_to, r))
            else:
                dispatch(r * 8 + at, z_to, r)

        each(do_pack)
        each(do_send)
        return c

    lax.fori_loop(0, 4, relay_pair, 0)
    for s in range(LOCAL * CAP):
        recv[5 * CAP + s] = send[5 * CAP + s]

    lax.fori_loop(4, 8, relay_pair, 0)
    def answer(k, z_to, r, sem):
        rows = pl.ds(k * CAP, CAP)
        device = (
            lax.rem(z_to, 8) * 16 + lax.rem(y + 4 - lax.rem(r, 4), 4) * 4
            + lax.rem(x + 4 - lax.div(r, 4), 4)
        )
        pltpu.make_async_remote_copy(
            src_ref=outb.at[rows], dst_ref=ret.at[rows], send_sem=rsend_sem,
            recv_sem=rrecv_sem.at[sem], device_id=(device, tp), device_id_type=MESH,
        ).start()

    def answers(g):
        def one(r, c):
            @pl.when(r >= 4)
            def _():
                answer(r * 8, z + 13 - 2 * lax.rem(r, 2), r, g)

            for at in range(1, 8):
                z_to = z + 8 - DZ[at] + (0 if at == 7 else 1 - 2 * (at % 2))
                if at >= 5 and g == 0:
                    pl.when(r > 0)(lambda at=at, z_to=z_to: answer(r * 8 + at, z_to, r, g))
                else:
                    answer(r * 8 + at, z_to, r, g)
            return c

        lax.fori_loop(g * 16 // GROUPS, (g + 1) * 16 // GROUPS, one, 0)

    for g in range(GROUPS):
        base = g * ROWS
        all_in(recv.at[pl.ds(0, (PER_GROUP - LOCAL * (g == 0)) * CAP)], recv_sem.at[g])

        for r in range(0, ROWS, 16):
            xg[r : r + 16, :] = recv[base + r : base + r + 16].reshape(16, SUB * LANES)

        for h, (gate_w, up_w) in enumerate(((wg, wu), (wgo, wuo))):
            if g == 0:
                if h == 0:
                    for copy in own:
                        copy.wait()
                else:
                    for copy in other:
                        copy.wait_recv()
            for t in range(2):
                cols = slice(t * 256, t * 256 + 256)
                hid[:, h * 512 + t * 256 : h * 512 + t * 256 + 256] = clamped_unit(
                    jnp.dot(xg[...], gate_w[:, cols], preferred_element_type=F32),
                    jnp.dot(xg[...], up_w[:, cols], preferred_element_type=F32),
                )

        for t in range(8):
            cols = slice(t * 256, t * 256 + 256)
            first = jnp.dot(hid[:, :512], wd[:, cols], preferred_element_type=F32).astype(BF16)
            second = jnp.dot(hid[:, 512:], wdo[:, cols], preferred_element_type=F32).astype(BF16)
            summed = first.astype(F32) + second.astype(F32)
            for i in range(2):
                acc[pl.ds(2 * t + i, ROWS, stride=SUB), :] = summed[:, i * LANES : (i + 1) * LANES]

        for r in range(0, ROWS, 16):
            outb[base + r : base + r + 16] = (
                acc[r * SUB : (r + 16) * SUB, :].reshape(16, SUB, LANES).astype(BF16)
            )

        answers(g)
        for r in range(4 if g == 0 else 0):
            answer(r * 8, z + 4, r, GROUPS)
    for s in range(LOCAL * CAP):
        ret[5 * CAP + s] = outb[5 * CAP + s]

    for i in range(2):
        ahead[4 + i].wait_recv()
        copy = pltpu.make_async_copy(sharen.at[i], weightn.at[i], weightn_sem.at[i])
        copy.start()
        copy.wait()
    all_in(ret.at[pl.ds(0, (PER_GROUP - LOCAL - 4) * CAP)], rrecv_sem.at[0])
    all_in(ret.at[pl.ds(0, 4 * CAP)], rrecv_sem.at[GROUPS])
    for g in range(1, GROUPS):
        all_in(ret.at[pl.ds(0, PER_GROUP * CAP)], rrecv_sem.at[g])

    def chosen_rows(t, index_of, weight_of, first):
        return weight_of[first, t] * ret[index_of[3, t]].astype(F32) + weight_of[
            first + 1, t
        ] * ret[index_of[4, t]].astype(F32)

    def send_part(j):
        rows = slice(j * CHUNK, (j + 1) * CHUNK)
        for i, d in enumerate((7, 1)):
            pltpu.make_async_remote_copy(
                src_ref=part.at[i, rows], dst_ref=pn.at[i, rows], send_sem=psend_sem.at[i],
                recv_sem=precv_sem.at[i, j], device_id=(chip(d, 0, 0), tp), device_id_type=MESH,
            ).start()

    def relay_sums(t, c):
        for i in range(2):
            part[i, t] = chosen_rows(t, indexn.at[i], weightn.at[i], 2 * i).astype(BF16)
        return c

    chunks = 128 // CHUNK
    for j in range(chunks):
        lax.fori_loop(j * CHUNK, (j + 1) * CHUNK, relay_sums, 0, unroll=4)
        if j > 0:
            send_part(j - 1)
    send_part(chunks - 1)

    all_in(third_all, drecv_sem.at[2])
    swap = pltpu.make_async_remote_copy(
        src_ref=dense.at[tp], dst_ref=dense.at[tp], send_sem=dsend_sem.at[3],
        recv_sem=drecv_sem.at[3], device_id=(me, 1 - tp), device_id_type=MESH,
    )
    swap.start()
    swap.wait_recv()

    pre = jnp.zeros((128, 256), F32)
    for i in range(8):
        pre = pre + jnp.dot(
            x2[:, i * 256 : (i + 1) * 256], dense[0, i].reshape(256, 256), preferred_element_type=F32
        )
    dense_hidden = jax.nn.silu(pre).astype(BF16)
    small[3].wait()
    gate = jax.nn.sigmoid(dgate[...])
    for i in range(8):
        piece = lax.dot_general(
            dense_hidden, dense[1, i].reshape(256, 256), (((1,), (1,)), ((), ())),
            preferred_element_type=F32,
        )
        for j in range(2):
            at = 2 * i + j
            branch[pl.ds(at, 128, stride=SUB), :] = (
                piece[:, j * LANES : (j + 1) * LANES] * gate[at : at + 1, :]
            )

    weight_copy.wait()

    def straight(t, c):
        tile = pl.ds(pl.multiple_of(t * SUB, SUB), SUB)
        acc[tile, :] = chosen_rows(t, index, weight, 4) + branch[tile, :]
        return c

    lax.fori_loop(0, 128, straight, 0, unroll=4)
    for j in range(chunks):
        rows = slice(j * CHUNK, (j + 1) * CHUNK)
        for i in range(2):
            all_in(pn.at[i, rows], precv_sem.at[i, j])
        total = (
            acc[j * CHUNK * SUB : (j + 1) * CHUNK * SUB, :].reshape(CHUNK, SUB, LANES)
            + pn[0, rows].astype(F32) + pn[1, rows].astype(F32)
        )
        o_ref[rows, :] = total.reshape(CHUNK, SUB * LANES).astype(BF16)

    all_in(send.at[pl.ds(0, (PEERS - LOCAL) * CAP)], send_sem)
    for copy in ahead:
        copy.wait_send()
    all_in(outb.at[pl.ds(0, (PEERS - LOCAL) * CAP)], rsend_sem)
    for i in range(2):
        all_in(part.at[i], psend_sem.at[i])
    for copy in other:
        copy.wait_send()
    all_in(z_all, dsend_sem.at[0])
    all_in(second_all, dsend_sem.at[1])
    all_in(third_all, dsend_sem.at[2])
    swap.wait_send()


def shards(
    tokens, norm_gain, routes, route_weights, w_gate, w_up, w_down, dense_in, dense_out, dense_gate
):
    hbm = pl.BlockSpec(memory_space=pl.ANY)
    dma = pltpu.SemaphoreType.DMA
    return pl.pallas_call(
        kernel,
        out_shape=jax.ShapeDtypeStruct((128, 2048), BF16),
        in_specs=[hbm] * 10,
        out_specs=pl.BlockSpec(memory_space=pltpu.VMEM),
        scratch_shapes=[
            pltpu.VMEM((2, 128), jnp.int32),
            pltpu.VMEM((1, 2048), F32),
            pltpu.VMEM((SUB, LANES), F32),
            pltpu.VMEM((8, 128), jnp.int32),
            pltpu.SMEM((8, 128), jnp.int32),
            pltpu.VMEM((2, 128), F32),
            pltpu.VMEM((2, 128, SUB, LANES), BF16),
            pltpu.VMEM((2, 8, 128), jnp.int32),
            pltpu.SMEM((2, 8, 128), jnp.int32),
            pltpu.VMEM((8, 128), F32),
            pltpu.VMEM((2, 8, 128), F32),
            pltpu.VMEM((2, 128, SUB, LANES), BF16),
            pltpu.VMEM((2, 128, SUB, LANES), BF16),
            pltpu.SMEM((8, 128), F32),
            pltpu.SMEM((2, 8, 128), F32),
            pltpu.VMEM((128, 2048), BF16),
            pltpu.VMEM((128, 2048), BF16),
            pltpu.VMEM((128, SUB, LANES), BF16),
            pltpu.VMEM((PEERS * CAP, SUB, LANES), BF16),
            pltpu.VMEM((PEERS * CAP, SUB, LANES), BF16),
            pltpu.VMEM((ROWS, 2048), BF16),
            pltpu.VMEM((ROWS, 1024), BF16),
            pltpu.VMEM((2048, LANES) if ROWS < 128 else (ROWS * SUB, LANES), F32),
            pltpu.VMEM((PEERS * CAP, SUB, LANES), BF16),
            pltpu.VMEM((PEERS * CAP, SUB, LANES), BF16),
            pltpu.VMEM((2048, 512), BF16),
            pltpu.VMEM((2048, 512), BF16),
            pltpu.VMEM((512, 2048), BF16),
            pltpu.VMEM((2048, 512), BF16),
            pltpu.VMEM((2048, 512), BF16),
            pltpu.VMEM((512, 2048), BF16),
            pltpu.VMEM((2, 8, 4, 4, 16, 256), BF16),
            pltpu.VMEM((128 * SUB, LANES), F32),
            dma((4,)), dma, pltpu.SemaphoreType.REGULAR, pltpu.SemaphoreType.REGULAR,
            dma((2,)), dma((2,)), dma((2,)), dma((2,)), dma((2,)),
            dma((2,)), dma((2,)), dma, dma((2,)), dma((2,)), dma((2, 128 // CHUNK)),
            dma, dma((3,)), dma((3,)), dma((3,)), dma, dma((4,)), dma((4,)),
            dma, dma((GROUPS,)), dma, dma((GROUPS + 1,)),
        ],
        compiler_params=pltpu.CompilerParams(
            collective_id=0, has_side_effects=True, vmem_limit_bytes=50 << 20
        ),
    )(
        *(
            pltpu.with_memory_space_constraint(operand, pltpu.HBM)
            for operand in (
                routes.T, route_weights.T, tokens, norm_gain.reshape(1, -1),
                dense_gate.reshape(SUB, LANES), w_gate[0], w_up[0], w_down[0], dense_in, dense_out,
            )
        )
    )


def solution(mesh):
    placed = (
        P(("ep", "tp"), None),
        P(),
        P(("ep", "tp"), None),
        P(("ep", "tp"), None),
        P("ep", None, "tp"),
        P("ep", None, "tp"),
        P("ep", "tp", None),
        P("ep", None),
        P("ep", None),
        P(),
    )
    return jax.shard_map(
        shards, mesh=mesh, in_specs=placed, out_specs=P(("ep", "tp"), None), check_vma=False
    )
```

```python
import jax
import jax.numpy as jnp
from jax import lax
from jax.experimental import pallas as pl
from jax.experimental.pallas import tpu as pltpu
from jax.sharding import PartitionSpec as P

CLAMP_LIMIT = 7.0
SLOPE_ALPHA = 1.702
NORM_EPS = 1e-06
MESH = pl.DeviceIdType.MESH
BF16 = jnp.bfloat16
F32 = jnp.float32

PEERS = 128
CAP = 3
LANES = 128
SUB = 16
SELF = 7
GROUPS = 4
PER_GROUP = PEERS // GROUPS
ROWS = PER_GROUP * CAP
LOCAL = 3
CHUNK = 16
DZ = (4, 5, 3, 6, 2, 7, 1, 0)


def place_of(dz, dy, dx):
    j = jnp.where(dz == 0, 0, jnp.where(dz <= 4, 2 * dz - 1, 2 * (8 - dz)))
    return (dx * 4 + dy) * 8 + 7 - j


def offset_of(k):
    j = 7 - lax.rem(k, 8)
    odd = lax.rem(j, 2)
    half = lax.div(j, 2)
    dz = lax.rem(odd * (half + 1) + (1 - odd) * (8 - half), 8)
    r = lax.div(k, 8)
    return dz, lax.rem(r, 4), lax.div(r, 4)


def clamped_unit(gate_pre, up_pre):
    gate_clip = jnp.minimum(gate_pre, CLAMP_LIMIT)
    up_clip = jnp.clip(up_pre, -CLAMP_LIMIT, CLAMP_LIMIT)
    return ((up_clip + 1.0) * gate_clip * jax.nn.sigmoid(SLOPE_ALPHA * gate_clip)).astype(BF16)


def kernel(
    routes_hbm, rw_hbm, tok_hbm, gain_hbm, dgate_hbm, wg_hbm, wu_hbm, wd_hbm, din_hbm, dout_hbm,
    o_ref,
    routes, gain, dgate, table, index, rw, far, xn, tn, indexn, share, sharen, part, pn, weight, weightn,
    tok, x2, x3, send, recv, xg, hid, acc, outb, ret, wg, wu, wd, wgo, wuo, wdo, dense, branch,
    small_sem, index_sem, y_sem, x_sem, nsend_sem, nrecv_sem, tsend_sem, trecv_sem, indexn_sem, ssend_sem, srecv_sem, weight_sem, weightn_sem, psend_sem, precv_sem,
    tok_sem, w_sem, wsend_sem, wrecv_sem, d_sem, dsend_sem, drecv_sem,
    send_sem, recv_sem, rsend_sem, rrecv_sem,
):
    me = lax.axis_index("ep")
    tp = lax.axis_index("tp")
    z, y, x = lax.div(me, 16), lax.rem(lax.div(me, 4), 4), lax.rem(me, 4)

    def chip(dz, dy, dx):
        return (
            lax.rem(z + dz, 8) * 16 + lax.rem(y + dy, 4) * 4 + lax.rem(x + dx, 4)
        )

    def back(dz, dy, dx):
        return (
            lax.rem(z + 8 - dz, 8) * 16 + lax.rem(y + 4 - dy, 4) * 4 + lax.rem(x + 4 - dx, 4)
        )

    small = [
        pltpu.make_async_copy(a, b, small_sem.at[i])
        for i, (a, b) in enumerate(
            ((routes_hbm, routes), (gain_hbm, gain), (rw_hbm, rw), (dgate_hbm, dgate))
        )
    ]
    tok_copy = pltpu.make_async_copy(tok_hbm, tok, tok_sem)
    small[0].start()
    tok_copy.start()

    for r in range(4):
        for s in range(CAP):
            ret[r * 8 * CAP + s] = jnp.zeros((SUB, LANES), BF16)

    def greet(sem, device):
        pl.semaphore_signal(sem, inc=1, device_id=device, device_id_type=MESH)

    barrier = pltpu.get_barrier_semaphore()
    for d in (4, 3, 5, 2, 6, 1, 7):
        greet(barrier, (chip(d, 0, 0), tp))
    for d in (2, 1, 3):
        greet(barrier, (chip(0, d, 0), tp))
        greet(barrier, (chip(0, 0, d), tp))
    greet(barrier, (me, 1 - tp))
    for copy in small[1:]:
        copy.start()

    @pl.when(tp == 0)
    def _():
        pltpu.make_async_copy(din_hbm, dense.at[0, z, y, x], d_sem).start()

    @pl.when(tp == 1)
    def _():
        pltpu.make_async_copy(dout_hbm, dense.at[1, z, y, x], d_sem).start()

    own = [
        pltpu.make_async_copy(a, b, w_sem.at[i])
        for i, (a, b) in enumerate(((wg_hbm, wg), (wu_hbm, wu), (wd_hbm, wd)))
    ]
    other = [
        pltpu.make_async_remote_copy(
            src_ref=a, dst_ref=b, send_sem=wsend_sem.at[i], recv_sem=wrecv_sem.at[i],
            device_id=(me, 1 - tp), device_id_type=MESH,
        )
        for i, (a, b) in enumerate(((wg_hbm, wgo), (wu_hbm, wuo), (wd_hbm, wdo)))
    ]

    table[...] = jnp.zeros_like(table)
    small[0].wait()
    tok_copy.wait()
    small[1].wait()
    chosen = routes[...]
    place = place_of(
        (lax.shift_right_logical(chosen, 4) - z) & 7,
        ((lax.shift_right_logical(chosen, 2) & 3) - y) & 3,
        ((chosen & 3) - x) & 3,
    )
    sub = lax.broadcasted_iota(jnp.int32, (PEERS, 128), 0)
    lane = lax.broadcasted_iota(jnp.int32, (PEERS, 128), 1)
    before = jnp.where(sub < lane, 1.0, 0.0).astype(BF16)
    token = lax.broadcasted_iota(jnp.int32, (8, 128), 1).astype(F32).astype(BF16)
    hits, slots = [], []
    for c in range(2):
        hit = jnp.where(sub == place[c : c + 1, :], 1.0, 0.0)
        earlier = jnp.dot(hit.astype(BF16), before, preferred_element_type=F32)
        if c == 1:
            earlier = earlier + jnp.sum(hits[0], axis=1, keepdims=True)
        slot = jnp.sum(hit * earlier, axis=0, keepdims=True)
        table[3 + c : 4 + c, :] = jnp.clip(
            place[c : c + 1, :] * CAP + slot.astype(jnp.int32), 0, PEERS * CAP - 1
        )
        table[5 + c : 6 + c, :] = jnp.clip(
            lax.shift_right_logical(place[c : c + 1, :], 3) * CAP + slot.astype(jnp.int32),
            0, 4 * CAP - 1,
        )
        hits.append(hit)
        slots.append(slot)
    for s in range(CAP):
        held = sum(jnp.where(slots[c] == s, hits[c], 0.0) for c in range(2)).astype(BF16)
        named = lax.dot_general(
            token, held, (((1,), (1,)), ((), ())), preferred_element_type=F32
        )
        table[s : s + 1, :] = jnp.clip(named[:1].astype(jnp.int32), 0, 127)
    index_copy = pltpu.make_async_copy(table, index, index_sem)
    index_copy.start()

    small[2].wait()
    at = place & 7
    flank = (at == 0) & (place >= 32)
    even = (lax.shift_right_logical(place, 3) & 1) == 0
    up = ((at == 2) | (at == 4) | (at == 6)) | (flank & even)
    down = ((at == 1) | (at == 3) | (at == 5)) | (flank & ~even)
    share[...] = jnp.zeros_like(share)
    share[0:2, :] = jnp.where(up, rw[...], 0.0)
    share[2:4, :] = jnp.where(down, rw[...], 0.0)
    share[4:6, :] = jnp.where(at == 7, rw[...], 0.0)
    share[6:8, :] = jnp.where((at == 0) & (place < 32), rw[...], 0.0)
    weight_copy = pltpu.make_async_copy(share, weight, weight_sem)
    weight_copy.start()

    for i in range(8):
        rows = slice(i * 16, i * 16 + 16)
        wide = tok[rows, :].astype(F32)
        scale = lax.rsqrt(jnp.mean(wide * wide, axis=1, keepdims=True) + NORM_EPS)
        normed = (wide * scale * gain[...]).astype(BF16)
        x2[rows, :] = normed
        x3[rows] = normed.reshape(16, SUB, LANES)
    def spread(stage, count, block, target):
        for d in range(1, count):
            pltpu.make_async_remote_copy(
                src_ref=block, dst_ref=block, send_sem=dsend_sem.at[stage],
                recv_sem=drecv_sem.at[stage], device_id=(target(d), tp), device_id_type=MESH,
            ).start()

    def along_y(d):
        return chip(0, d, 0)

    def along_x(d):
        return chip(0, 0, d)

    z_all = dense.at[tp, pl.ds(0, 7), y, x]
    second_all = dense.at[tp, :, pl.ds(0, 3), x]
    third_all = dense.at[tp, :, :, pl.ds(0, 3)]

    def all_in(ref, sem):
        pltpu.make_async_copy(ref, ref, sem).wait()

    pltpu.make_async_copy(din_hbm, dense.at[tp, z, y, x], d_sem).wait()
    pl.semaphore_wait(barrier, 14)
    spread(0, 8, dense.at[tp, z, y, x], lambda d: chip(d, 0, 0))
    ahead = [
        pltpu.make_async_remote_copy(
            src_ref=a, dst_ref=b.at[i], send_sem=ss.at[i], recv_sem=rs.at[i],
            device_id=(chip(d, 0, 0), tp), device_id_type=MESH,
        )
        for a, b, ss, rs in (
            (table, tn, tsend_sem, trecv_sem), (x3, xn, nsend_sem, nrecv_sem),
            (share, sharen, ssend_sem, srecv_sem),
        )
        for i, d in enumerate((1, 7))
    ]
    for copy in ahead:
        copy.start()
    for d in (2, 1, 3):
        greet(y_sem, (chip(0, d, 0), tp))
    index_copy.wait()

    def pack(k, rows_of, index_of):
        for s in range(CAP):
            send[k * CAP + s] = rows_of[index_of[s, k]]

    def dispatch(k, z_to, r):
        rows = pl.ds(k * CAP, CAP)
        device = z_to * 16 + lax.rem(y + lax.rem(r, 4), 4) * 4 + lax.rem(x + lax.div(r, 4), 4)
        pltpu.make_async_remote_copy(
            src_ref=send.at[rows], dst_ref=recv.at[rows], send_sem=send_sem,
            recv_sem=recv_sem.at[lax.div(k, PER_GROUP)],
            device_id=(device, tp), device_id_type=MESH,
        ).start()

    for r in range(4):
        pack(r * 8, x3, index)
    pl.semaphore_wait(y_sem, 3)
    for d in (2, 1, 3):
        greet(x_sem, (chip(0, 0, d), tp))
    for r in range(4):
        dispatch(r * 8, lax.rem(z + 4, 8), r)

    def pack_flat(r, c):
        pack(r * 8 + 7, x3, index)
        return c

    def dispatch_flat(r, c):
        dispatch(r * 8 + 7, z, r)
        return c

    lax.fori_loop(0, 16, pack_flat, 0)
    pl.semaphore_wait(x_sem, 3)
    lax.fori_loop(1, 16, dispatch_flat, 0)
    for copy in own:
        copy.start()
    for copy in other:
        copy.start()

    all_in(z_all, drecv_sem.at[0])

    @pl.when(tp == 0)
    def _():
        spread(1, 4, dense.at[0, :, y, x], along_y)

    @pl.when(tp == 1)
    def _():
        spread(1, 4, dense.at[1, :, y, x], along_x)

    all_in(second_all, drecv_sem.at[1])

    @pl.when(tp == 0)
    def _():
        spread(2, 4, dense.at[0, :, :, x], along_x)

    @pl.when(tp == 1)
    def _():
        spread(2, 4, dense.at[1, :, y], along_y)

    onward = []
    for i in range(2):
        ahead[i].wait_recv()
        onward.append(pltpu.make_async_copy(tn.at[i], indexn.at[i], indexn_sem.at[i]))
        onward[i].start()
    for i in range(2):
        onward[i].wait()
    for i in range(2):
        ahead[2 + i].wait_recv()

    def relay_pair(h, c):
        def each(visit):
            for p in range(2):
                r = 2 * h + p
                for at in range(7):
                    if at == 0:
                        pl.when(h >= 2)(lambda r=r, p=p: visit(r, 0, p, False))
                    else:
                        visit(r, at, at % 2, p == 0 and at >= 5)

        def do_pack(r, at, i, local):
            pack(r * 8 + at, xn.at[i], indexn.at[i])

        def do_send(r, at, i, local):
            z_to = lax.rem(z + (7 if i == 0 else 1) + DZ[at], 8)
            if local:
                pl.when(h > 0)(lambda: dispatch(r * 8 + at, z_to, r))
            else:
                dispatch(r * 8 + at, z_to, r)

        each(do_pack)
        each(do_send)
        return c

    lax.fori_loop(0, 4, relay_pair, 0)
    for s in range(LOCAL * CAP):
        recv[5 * CAP + s] = send[5 * CAP + s]

    lax.fori_loop(4, 8, relay_pair, 0)
    def answer(k, z_to, r, sem, into=None):
        rows = pl.ds(k * CAP, CAP)
        device = (
            lax.rem(z_to, 8) * 16 + lax.rem(y + 4 - lax.rem(r, 4), 4) * 4
            + lax.rem(x + 4 - lax.div(r, 4), 4)
        )
        pltpu.make_async_remote_copy(
            src_ref=outb.at[rows], dst_ref=ret.at[rows] if into is None else into, send_sem=rsend_sem,
            recv_sem=rrecv_sem.at[sem], device_id=(device, tp), device_id_type=MESH,
        ).start()

    def answers(g):
        def one(r, c):
            @pl.when(r >= 4)
            def _():
                answer(r * 8, z + 13 - 2 * lax.rem(r, 2), r, g)

            for at in range(1, 8):
                z_to = z + 8 - DZ[at] + (0 if at == 7 else 1 - 2 * (at % 2))
                if at >= 5 and g == 0:
                    pl.when(r > 0)(lambda at=at, z_to=z_to: answer(r * 8 + at, z_to, r, g))
                else:
                    answer(r * 8 + at, z_to, r, g)
            return c

        lax.fori_loop(g * 16 // GROUPS, (g + 1) * 16 // GROUPS, one, 0)

    for g in range(GROUPS):
        base = g * ROWS
        all_in(recv.at[pl.ds(0, (PER_GROUP - LOCAL * (g == 0)) * CAP)], recv_sem.at[g])

        for r in range(0, ROWS, 16):
            xg[r : r + 16, :] = recv[base + r : base + r + 16].reshape(16, SUB * LANES)

        for h, (gate_w, up_w) in enumerate(((wg, wu), (wgo, wuo))):
            if g == 0:
                if h == 0:
                    for copy in own:
                        copy.wait()
                else:
                    for copy in other:
                        copy.wait_recv()
            for t in range(2):
                cols = slice(t * 256, t * 256 + 256)
                hid[:, h * 512 + t * 256 : h * 512 + t * 256 + 256] = clamped_unit(
                    jnp.dot(xg[...], gate_w[:, cols], preferred_element_type=F32),
                    jnp.dot(xg[...], up_w[:, cols], preferred_element_type=F32),
                )

        for t in range(8):
            cols = slice(t * 256, t * 256 + 256)
            first = jnp.dot(hid[:, :512], wd[:, cols], preferred_element_type=F32).astype(BF16)
            second = jnp.dot(hid[:, 512:], wdo[:, cols], preferred_element_type=F32).astype(BF16)
            summed = first.astype(F32) + second.astype(F32)
            for i in range(2):
                acc[pl.ds(2 * t + i, ROWS, stride=SUB), :] = summed[:, i * LANES : (i + 1) * LANES]

        for r in range(0, ROWS, 16):
            outb[base + r : base + r + 16] = (
                acc[r * SUB : (r + 16) * SUB, :].reshape(16, SUB, LANES).astype(BF16)
            )

        answers(g)
    for r in range(4):
        answer(r * 8, z + 4, r, GROUPS, far.at[pl.ds(r * CAP, CAP)])
    for s in range(LOCAL * CAP):
        ret[5 * CAP + s] = outb[5 * CAP + s]

    for i in range(2):
        ahead[4 + i].wait_recv()
        copy = pltpu.make_async_copy(sharen.at[i], weightn.at[i], weightn_sem.at[i])
        copy.start()
        copy.wait()
    all_in(ret.at[pl.ds(0, (PER_GROUP - LOCAL - 4) * CAP)], rrecv_sem.at[0])
    for g in range(1, GROUPS):
        all_in(ret.at[pl.ds(0, PER_GROUP * CAP)], rrecv_sem.at[g])

    def chosen_rows(t, index_of, weight_of, first):
        return weight_of[first, t] * ret[index_of[3, t]].astype(F32) + weight_of[
            first + 1, t
        ] * ret[index_of[4, t]].astype(F32)

    def send_part(j):
        rows = slice(j * CHUNK, (j + 1) * CHUNK)
        for i, d in enumerate((7, 1)):
            pltpu.make_async_remote_copy(
                src_ref=part.at[i, rows], dst_ref=pn.at[i, rows], send_sem=psend_sem.at[i],
                recv_sem=precv_sem.at[i, j], device_id=(chip(d, 0, 0), tp), device_id_type=MESH,
            ).start()

    def relay_sums(t, c):
        for i in range(2):
            part[i, t] = chosen_rows(t, indexn.at[i], weightn.at[i], 2 * i).astype(BF16)
        return c

    chunks = 128 // CHUNK
    for j in range(chunks):
        lax.fori_loop(j * CHUNK, (j + 1) * CHUNK, relay_sums, 0, unroll=4)
        if j > 0:
            send_part(j - 1)
    send_part(chunks - 1)

    all_in(third_all, drecv_sem.at[2])
    swap = pltpu.make_async_remote_copy(
        src_ref=dense.at[tp], dst_ref=dense.at[tp], send_sem=dsend_sem.at[3],
        recv_sem=drecv_sem.at[3], device_id=(me, 1 - tp), device_id_type=MESH,
    )
    swap.start()
    swap.wait_recv()

    pre = jnp.zeros((128, 256), F32)
    for i in range(8):
        pre = pre + jnp.dot(
            x2[:, i * 256 : (i + 1) * 256], dense[0, i].reshape(256, 256), preferred_element_type=F32
        )
    dense_hidden = jax.nn.silu(pre).astype(BF16)
    small[3].wait()
    gate = jax.nn.sigmoid(dgate[...])
    for i in range(8):
        piece = lax.dot_general(
            dense_hidden, dense[1, i].reshape(256, 256), (((1,), (1,)), ((), ())),
            preferred_element_type=F32,
        )
        for j in range(2):
            at = 2 * i + j
            branch[pl.ds(at, 128, stride=SUB), :] = (
                piece[:, j * LANES : (j + 1) * LANES] * gate[at : at + 1, :]
            )

    weight_copy.wait()
    all_in(far, rrecv_sem.at[GROUPS])

    def straight(t, c):
        tile = pl.ds(pl.multiple_of(t * SUB, SUB), SUB)
        from_far = weight[6, t] * far[index[5, t]].astype(F32) + weight[7, t] * far[
            index[6, t]
        ].astype(F32)
        acc[tile, :] = chosen_rows(t, index, weight, 4) + from_far + branch[tile, :]
        return c

    lax.fori_loop(0, 128, straight, 0, unroll=4)
    for j in range(chunks):
        rows = slice(j * CHUNK, (j + 1) * CHUNK)
        for i in range(2):
            all_in(pn.at[i, rows], precv_sem.at[i, j])
        total = (
            acc[j * CHUNK * SUB : (j + 1) * CHUNK * SUB, :].reshape(CHUNK, SUB, LANES)
            + pn[0, rows].astype(F32) + pn[1, rows].astype(F32)
        )
        o_ref[rows, :] = total.reshape(CHUNK, SUB * LANES).astype(BF16)

    all_in(send.at[pl.ds(0, (PEERS - LOCAL) * CAP)], send_sem)
    for copy in ahead:
        copy.wait_send()
    all_in(outb.at[pl.ds(0, (PEERS - LOCAL) * CAP)], rsend_sem)
    for i in range(2):
        all_in(part.at[i], psend_sem.at[i])
    for copy in other:
        copy.wait_send()
    all_in(z_all, dsend_sem.at[0])
    all_in(second_all, dsend_sem.at[1])
    all_in(third_all, dsend_sem.at[2])
    swap.wait_send()


def shards(
    tokens, norm_gain, routes, route_weights, w_gate, w_up, w_down, dense_in, dense_out, dense_gate
):
    hbm = pl.BlockSpec(memory_space=pl.ANY)
    dma = pltpu.SemaphoreType.DMA
    return pl.pallas_call(
        kernel,
        out_shape=jax.ShapeDtypeStruct((128, 2048), BF16),
        in_specs=[hbm] * 10,
        out_specs=pl.BlockSpec(memory_space=pltpu.VMEM),
        scratch_shapes=[
            pltpu.VMEM((2, 128), jnp.int32),
            pltpu.VMEM((1, 2048), F32),
            pltpu.VMEM((SUB, LANES), F32),
            pltpu.VMEM((8, 128), jnp.int32),
            pltpu.SMEM((8, 128), jnp.int32),
            pltpu.VMEM((2, 128), F32),
            pltpu.VMEM((4 * CAP, SUB, LANES), BF16),
            pltpu.VMEM((2, 128, SUB, LANES), BF16),
            pltpu.VMEM((2, 8, 128), jnp.int32),
            pltpu.SMEM((2, 8, 128), jnp.int32),
            pltpu.VMEM((8, 128), F32),
            pltpu.VMEM((2, 8, 128), F32),
            pltpu.VMEM((2, 128, SUB, LANES), BF16),
            pltpu.VMEM((2, 128, SUB, LANES), BF16),
            pltpu.SMEM((8, 128), F32),
            pltpu.SMEM((2, 8, 128), F32),
            pltpu.VMEM((128, 2048), BF16),
            pltpu.VMEM((128, 2048), BF16),
            pltpu.VMEM((128, SUB, LANES), BF16),
            pltpu.VMEM((PEERS * CAP, SUB, LANES), BF16),
            pltpu.VMEM((PEERS * CAP, SUB, LANES), BF16),
            pltpu.VMEM((ROWS, 2048), BF16),
            pltpu.VMEM((ROWS, 1024), BF16),
            pltpu.VMEM((2048, LANES) if ROWS < 128 else (ROWS * SUB, LANES), F32),
            pltpu.VMEM((PEERS * CAP, SUB, LANES), BF16),
            pltpu.VMEM((PEERS * CAP, SUB, LANES), BF16),
            pltpu.VMEM((2048, 512), BF16),
            pltpu.VMEM((2048, 512), BF16),
            pltpu.VMEM((512, 2048), BF16),
            pltpu.VMEM((2048, 512), BF16),
            pltpu.VMEM((2048, 512), BF16),
            pltpu.VMEM((512, 2048), BF16),
            pltpu.VMEM((2, 8, 4, 4, 16, 256), BF16),
            pltpu.VMEM((128 * SUB, LANES), F32),
            dma((4,)), dma, pltpu.SemaphoreType.REGULAR, pltpu.SemaphoreType.REGULAR,
            dma((2,)), dma((2,)), dma((2,)), dma((2,)), dma((2,)),
            dma((2,)), dma((2,)), dma, dma((2,)), dma((2,)), dma((2, 128 // CHUNK)),
            dma, dma((3,)), dma((3,)), dma((3,)), dma, dma((4,)), dma((4,)),
            dma, dma((GROUPS,)), dma, dma((GROUPS + 1,)),
        ],
        compiler_params=pltpu.CompilerParams(
            collective_id=0, has_side_effects=True, vmem_limit_bytes=50 << 20
        ),
    )(
        *(
            pltpu.with_memory_space_constraint(operand, pltpu.HBM)
            for operand in (
                routes.T, route_weights.T, tokens, norm_gain.reshape(1, -1),
                dense_gate.reshape(SUB, LANES), w_gate[0], w_up[0], w_down[0], dense_in, dense_out,
            )
        )
    )


def solution(mesh):
    placed = (
        P(("ep", "tp"), None),
        P(),
        P(("ep", "tp"), None),
        P(("ep", "tp"), None),
        P("ep", None, "tp"),
        P("ep", None, "tp"),
        P("ep", "tp", None),
        P("ep", None),
        P("ep", None),
        P(),
    )
    return jax.shard_map(
        shards, mesh=mesh, in_specs=placed, out_specs=P(("ep", "tp"), None), check_vma=False
    )
```
